256 devices in a mesh: row: 32 (over z, y), col: 8 (over x, core).
Axes of the slice: x: 4, y: 4, z: 8, core: 2. Of those that a mesh axis runs over, the one named last changes fastest.
Arguments:
- tokens: bfloat16 [2, 65536, 1024], P(None, 'row'), may hold values from -6 to 6
- norm_gain: float32 [1024], replicated, may hold values from 0.1 to 1.9
- w_fourier_in: bfloat16 [1024, 512], P(None, 'col'), may hold values from -0.1875 to 0.1875
- w_gate: bfloat16 [1024, 1024], replicated, may hold values from -0.1875 to 0.1875
- w_spectrum: bfloat16 [512, 1024], replicated, may hold values from -0.25 to 0.25
- w_output: bfloat16 [1024, 1024], P(None, 'col'), may hold values from -0.375 to 0.375
Outputs:
- block_output: bfloat16 [2, 65536, 1024], P(None, 'row', 'col')
The draws below stay inside these ranges and needn't reach their ends.
All inputs are finite; a program needn't handle non-finite values.
Results may differ from the reference program's by a relative error of at most 0.015.
Values may be sent and summed in bfloat16 or wider, within the bound.
A program may use at most 320 MiB of HBM per device.

```python
import jax
import jax.numpy as jnp
from jax import lax

D = 1024
GROUPS = 8
GROUP_WIDTH = 64
FOURIER_WIDTH = 512
SEQS = 2
SEQ = 65536


def block_scale(stream_key, dims, cuts, low, largest):
    gain, own = 1.0, jax.random.fold_in(stream_key, 6)
    for axis_at, parts in cuts:
        steps = jnp.exp(jax.random.uniform(jax.random.fold_in(own, axis_at), (parts,), jnp.float32, low / len(cuts), largest / len(cuts)))
        gain = gain * jnp.repeat(steps, dims[axis_at] // parts).reshape([-1 if axis == axis_at else 1 for axis in range(len(dims))])
    return gain


def normal_values(own_key, dims, spread, bound, split=(), held_as=jnp.bfloat16):
    values = jax.random.normal(own_key, dims, jnp.float32) * spread
    if len(split) > 0:
        values = block_scale(own_key, dims, split, -0.22, 0.18) * values
    return jnp.clip(values, min=-bound, max=bound).astype(held_as)


def setup_inputs(seed: int = 0) -> dict:
    key_list = jax.random.split(jax.random.key(seed), 7)
    return {
        "tokens": normal_values(key_list[0], (SEQS, SEQ, D), 1.0, 6.0, ((1, 32),)),
        "norm_gain": jnp.clip(1.0 + 0.18 * jax.random.normal(key_list[1], (D,), jnp.float32), 0.1, 1.9),
        "w_fourier_in": normal_values(key_list[2], (D, FOURIER_WIDTH), D ** -0.5, 0.1875, ((1, 8),)),
        "w_gate": normal_values(key_list[3], (D, D), D ** -0.5, 0.1875),
        "w_spectrum": normal_values(key_list[4], (FOURIER_WIDTH, D), FOURIER_WIDTH ** -0.5, 0.25),
        "w_output": normal_values(key_list[5], (D, D), (D // 4) ** -0.5, 0.375, ((1, 8),)),
    }


norm_eps = 1e-6


def reference(tokens, norm_gain, w_fourier_in, w_gate, w_spectrum, w_output):
    widened = tokens.astype(jnp.float32)
    inverse = lax.rsqrt(jnp.mean(widened * widened, axis=-1, keepdims=True) + norm_eps)
    normed = (widened * inverse * norm_gain).astype(jnp.bfloat16).reshape(SEQS * SEQ, D)
    fourier_in = jnp.dot(normed, w_fourier_in, preferred_element_type=jnp.float32).astype(jnp.bfloat16)
    grouped = fourier_in.astype(jnp.float32).reshape(SEQS, SEQ, GROUPS, GROUP_WIDTH)
    spectrum = jnp.real(jnp.fft.fft2(grouped, axes=(1, 3), norm="ortho")).astype(jnp.bfloat16)
    spectrum = spectrum.reshape(SEQS * SEQ, FOURIER_WIDTH)
    mixed_pre = jnp.dot(spectrum, w_spectrum, preferred_element_type=jnp.float32).astype(jnp.bfloat16)
    gate_pre = jnp.dot(normed, w_gate, preferred_element_type=jnp.float32)
    mixed = (jax.nn.sigmoid(gate_pre) * mixed_pre.astype(jnp.float32)).astype(jnp.bfloat16)
    block_output = jnp.dot(mixed, w_output, preferred_element_type=jnp.float32).astype(jnp.bfloat16)
    return block_output.reshape(SEQS, SEQ, D)
```

```python
import numpy as np
import jax
import jax.numpy as jnp
from jax import lax
from jax.experimental import pallas as pl
from jax.experimental.pallas import tpu as pltpu
from jax.sharding import PartitionSpec as P

MESH = pl.DeviceIdType.MESH
ROWS, COLS = 32, 8
SEQS, LOCAL, D = 2, 2048, 1024
TILE = 256
TILES = LOCAL // TILE
SEQ = ROWS * LOCAL
WIDTH = 64
CHANNELS = COLS * WIDTH
OUT = D // COLS
EPS = 1e-6
F32, BF16 = jnp.float32, jnp.bfloat16


def partner_channel(r, second):
    if r == 0:
        return 32 * second
    return WIDTH - r if second else r


def tables():
    n = np.arange(WIDTH)[:, None]
    analysis = np.zeros((2 * WIDTH, WIDTH))
    for r in range(ROWS):
        analysis[2 * r] = np.cos(2 * np.pi * n[:, 0] * r / WIDTH)
        analysis[2 * r + 1] = np.sin(2 * np.pi * n[:, 0] * r / WIDTH) if r else np.cos(np.pi * n[:, 0])
    a = np.arange(256)[:, None]
    p = np.arange(256)[None, :]
    turn = 2 * np.pi * (a * p % 256) / 256
    first = np.zeros((ROWS, 2, TILES, 4, 256))
    for e in range(2):
        first[:, e, :, 2 * e] = np.cos(turn).reshape(ROWS, TILES, 256)
        first[:, e, :, 2 * e + 1] = -np.sin(turn).reshape(ROWS, TILES, 256)
    first = first.reshape(2 * ROWS * TILES, 4 * 256)
    twist = 2 * np.pi * (a * p) / SEQ
    twist = np.concatenate([np.cos(twist), -np.sin(twist)], axis=1)
    second = np.concatenate([np.cos(turn), np.sin(turn)], axis=1) / np.sqrt(SEQ * WIDTH)
    select = np.zeros((CHANNELS, CHANNELS))
    for r in range(ROWS):
        for ch in range(2):
            for c in range(COLS):
                select[r * 16 + ch * 8 + c, c * WIDTH + partner_channel(r, ch)] = 1.0
    return (
        jnp.asarray(analysis, BF16),
        jnp.asarray(first, BF16),
        jnp.asarray(twist, F32),
        jnp.asarray(second, BF16),
        jnp.asarray(select, BF16),
    )


def dot(x, y, dims=((1,), (0,))):
    return lax.dot_general(x, y, (dims, ((), ())), preferred_element_type=F32)


def kernel(
    tokens, gain, w_in, w_gate, w_spec, w_out, analysis, first, twist, second, select,
    out,
    tok, gain_v, w_in_v, wc, w_gate_v, w_spec_v, w_map, w_out_v,
    analysis_v, first_v, twist_v, second_v, select_v,
    turned, send1, recv1, mid, both, sendx, recvx, wide, send2, recv2, sig, result,
    tok_sem, load_sem, s1, r1, sx, rx, s2, r2, so, ro, own_o, sw, rw, sf, rf,
):
    row, col = lax.axis_index("row"), lax.axis_index("col")
    chip, core = col // 2, col % 2

    barrier = pltpu.get_barrier_semaphore()

    def greet_row(d, _):
        pl.semaphore_signal(barrier, inc=1, device_id=((row + d) % ROWS, col), device_id_type=MESH)
        return 0

    def greet_col(d, _):
        pl.semaphore_signal(barrier, inc=1, device_id=(row, (col + d) % COLS), device_id_type=MESH)
        return 0

    lax.fori_loop(1, ROWS, greet_row, 0)
    lax.fori_loop(1, COLS, greet_col, 0)

    def cols_of(c):
        return pl.ds(pl.multiple_of(c * OUT, OUT), OUT)

    loads = [
        pltpu.make_async_copy(src, dst, load_sem.at[i])
        for i, (src, dst) in enumerate(
            [
                (analysis, analysis_v), (w_in, w_in_v), (gain, gain_v),
                (first, first_v), (twist, twist_v), (second, second_v),
                (w_gate, w_gate_v), (w_out, w_out_v.at[:, cols_of(col)]),
                (w_spec, w_spec_v), (select, select_v),
            ]
        )
    ]

    def tile_copy(b, j):
        return pltpu.make_async_copy(
            tokens.at[b, pl.ds(pl.multiple_of(j * TILE, TILE), TILE)], tok.at[b, j], tok_sem.at[b, j]
        )

    for i in range(3):
        loads[i].start()
    for b in range(SEQS):
        for j in range(TILES):
            tile_copy(b, j).start()
    for i in range(3, 10):
        loads[i].start()

    for i in range(3):
        loads[i].wait()
    folded = dot(analysis_v[...], w_in_v[...], ((1,), (1,))) * gain_v[...]
    wc[...] = jnp.transpose(folded).astype(BF16)

    def rows16(r):
        return pl.ds(pl.multiple_of(16 * r, 16), 16)

    def strided(ref, lo, hi, count, stride):
        halves = [
            jnp.concatenate([ref[h, pl.ds(at, count, stride), :] for at in (lo, hi)], axis=0) for h in range(2)
        ]
        return jnp.concatenate(halves, axis=1).astype(BF16)

    def project(b):
        def tile(j, _):
            tile_copy(b, j).wait()
            t = tok[b, j]
            wide_t = t.astype(F32)
            inverse = lax.rsqrt(jnp.sum(wide_t * wide_t, axis=1, keepdims=True) * (1.0 / D) + EPS)
            y = dot(t, wc[...]) * inverse
            flipped = jnp.transpose(y)[:WIDTH]
            for h in range(2):
                turned[h, pl.ds(pl.multiple_of(j * WIDTH, WIDTH), WIDTH), :] = flipped[:, 128 * h : 128 * (h + 1)]
            return 0

        lax.fori_loop(0, TILES, tile, 0)

        def pick(r, _):
            send1[b, rows16(r), :] = strided(turned, 2 * r, 2 * r + 1, TILES, WIDTH)
            return 0

        lax.fori_loop(0, ROWS, pick, 0)

    def row_copy(src, dst, ssem, rsem, b, peer):
        return pltpu.make_async_remote_copy(
            src_ref=src.at[b, rows16(peer)], dst_ref=dst.at[b, rows16(row)],
            send_sem=ssem.at[b], recv_sem=rsem.at[b], device_id=(peer, col), device_id_type=MESH,
        )

    def row_send(src, dst, ssem, rsem, b):
        def one(d, _):
            row_copy(src, dst, ssem, rsem, b, (row + d) % ROWS).start()
            return 0

        lax.fori_loop(1, ROWS, one, 0)
        dst[b, rows16(row), :] = src[b, rows16(row), :]

    def wait_bytes(ref, sem):
        pltpu.make_async_copy(ref, ref, sem).wait()

    most = pl.ds(0, 16 * (ROWS - 1))

    def col_send(b):
        def one(d, _):
            peer = (col + d) % COLS
            pltpu.make_async_remote_copy(
                src_ref=sendx.at[b, peer], dst_ref=recvx.at[b, col],
                send_sem=sx.at[b], recv_sem=rx.at[b], device_id=(row, peer), device_id_type=MESH,
            ).start()
            return 0

        lax.fori_loop(1, COLS, one, 0)
        recvx[b, col] = sendx[b, col]

    def fourier(b):
        wait_bytes(recv1.at[b, most], r1.at[b])
        y = dot(recv1[b], first_v[...], ((0,), (0,)))
        tr, ti = twist_v[:, :256], twist_v[:, 256:]
        ar, ai, br, bi = (y[:, 256 * i : 256 * (i + 1)] for i in range(4))
        pa, qa = ar * tr - ai * ti, ar * ti + ai * tr
        pb, qb = br * tr - bi * ti, br * ti + bi * tr
        lone = row == 0
        both[:256, :256] = pa.astype(BF16)
        both[256:, :256] = qa.astype(BF16)
        both[:256, 256:] = jnp.where(lone, pb, -qb).astype(BF16)
        both[256:, 256:] = jnp.where(lone, qb, pb).astype(BF16)
        d = dot(second_v[...], both[...])
        da, db = d[:, :256], d[:, 256:]
        made = (jnp.where(lone, da, da - db), jnp.where(lone, db, da + db))
        for ch in range(2):
            for h in range(2):
                mid[h, 256 * ch : 256 * (ch + 1)] = made[ch][:, 128 * h : 128 * (h + 1)]

        def pick(c, _):
            sendx[b, c] = strided(mid, c, 256 + c, ROWS, COLS)
            return 0

        lax.fori_loop(0, COLS, pick, 0)

    def regroup(b):
        wait_bytes(recvx.at[b, pl.ds(0, COLS - 1)], rx.at[b])

        def widen(c, _):
            block = recvx[b, c].astype(F32)
            for h in range(2):
                wide[h, pl.ds(pl.multiple_of(c * WIDTH, WIDTH), WIDTH), :] = block[:, 128 * h : 128 * (h + 1)]
            return 0

        lax.fori_loop(0, COLS, widen, 0)

        def pick(r, _):
            send2[b, rows16(r), :] = strided(wide, r, ROWS + r, COLS, WIDTH)
            return 0

        lax.fori_loop(0, ROWS, pick, 0)

    def gates(b):
        t = tok[b, col].astype(F32)
        inverse = lax.rsqrt(jnp.sum(t * t, axis=1, keepdims=True) * (1.0 / D) + EPS)
        normed = (t * inverse * gain_v[...]).astype(BF16)
        sig[b] = jax.nn.sigmoid(dot(normed, w_gate_v[...]))

    def share_out(d):
        peer = ((chip + d) % 4) * 2 + core
        return pltpu.make_async_remote_copy(
            src_ref=w_out_v.at[:, cols_of(col)], dst_ref=w_out_v.at[:, cols_of(col)],
            send_sem=sw, recv_sem=rw, device_id=(row, peer), device_id_type=MESH,
        )

    def pass_out(d):
        held = cols_of(((chip + d) % 4) * 2 + core)
        return pltpu.make_async_remote_copy(
            src_ref=w_out_v.at[:, held], dst_ref=w_out_v.at[:, held],
            send_sem=sf, recv_sem=rf, device_id=(row, chip * 2 + 1 - core), device_id_type=MESH,
        )

    def finish(b):
        wait_bytes(recv2.at[b, most], r2.at[b])
        pre = dot(recv2[b], w_map[...], ((0,), (0,))).astype(BF16).astype(F32)
        mixed = (sig[b] * pre).astype(BF16)
        result[b] = dot(mixed, w_out_v[...]).astype(BF16)
        place = pl.ds(pl.multiple_of(col * TILE, TILE), TILE)

        def one(d, _):
            peer = (col + d) % COLS
            pltpu.make_async_remote_copy(
                src_ref=result.at[b, :, cols_of(peer)], dst_ref=out.at[b, place],
                send_sem=so.at[b], recv_sem=ro.at[b], device_id=(row, peer), device_id_type=MESH,
            ).start()
            return 0

        lax.fori_loop(1, COLS, one, 0)
        pltpu.make_async_copy(result.at[b, :, cols_of(col)], out.at[b, place], own_o.at[b]).start()

    project(0)
    pl.semaphore_wait(barrier, ROWS - 1 + COLS - 1)
    row_send(send1, recv1, s1, r1, 0)
    project(1)
    row_send(send1, recv1, s1, r1, 1)

    loads[7].wait()
    for d in range(1, 4):
        share_out(d).start()
    pass_out(0).start()

    loads[6].wait()
    gates(0)
    gates(1)
    loads[8].wait()
    loads[9].wait()
    w_map[...] = dot(select_v[...], w_spec_v[...]).astype(BF16)

    for i in range(3, 6):
        loads[i].wait()
    fourier(0)
    col_send(0)
    regroup(0)
    row_send(send2, recv2, s2, r2, 0)
    fourier(1)
    col_send(1)

    shard = w_out_v.at[:, pl.ds(0, 3 * OUT)]
    wait_bytes(shard, rw)
    for d in range(1, 4):
        pass_out(d).start()

    regroup(1)
    row_send(send2, recv2, s2, r2, 1)
    wait_bytes(w_out_v.at[:, pl.ds(0, 4 * OUT)], rf)
    finish(0)
    finish(1)

    wait_bytes(shard, sw)
    wait_bytes(w_out_v.at[:, pl.ds(0, 4 * OUT)], sf)
    for b in range(SEQS):
        wait_bytes(send1.at[b, most], s1.at[b])
        wait_bytes(sendx.at[b, pl.ds(0, COLS - 1)], sx.at[b])
        wait_bytes(send2.at[b, most], s2.at[b])
        wait_bytes(result.at[b, :, pl.ds(0, (COLS - 1) * OUT)], so.at[b])
        wait_bytes(out.at[b, pl.ds(0, (COLS - 1) * TILE)], ro.at[b])
        wait_bytes(result.at[b, :, pl.ds(0, OUT)], own_o.at[b])


def on_device(tokens, norm_gain, w_fourier_in, w_gate, w_spectrum, w_output):
    dma = pltpu.SemaphoreType.DMA
    pair = dma((SEQS,))
    scratch = [
        pltpu.VMEM((SEQS, TILES, TILE, D), BF16),
        pltpu.VMEM((1, D), F32),
        pltpu.VMEM((D, WIDTH), BF16),
        pltpu.VMEM((D, 2 * WIDTH), BF16),
        pltpu.VMEM((D, D), BF16),
        pltpu.VMEM((CHANNELS, D), BF16),
        pltpu.VMEM((CHANNELS, D), BF16),
        pltpu.VMEM((D, D), BF16),
        pltpu.VMEM((2 * WIDTH, WIDTH), BF16),
        pltpu.VMEM((512, 1024), BF16),
        pltpu.VMEM((256, 512), F32),
        pltpu.VMEM((256, 512), BF16),
        pltpu.VMEM((CHANNELS, CHANNELS), BF16),
        pltpu.VMEM((2, TILES * WIDTH, 128), F32),
        pltpu.VMEM((SEQS, 16 * ROWS, 256), BF16),
        pltpu.VMEM((SEQS, 16 * ROWS, 256), BF16),
        pltpu.VMEM((2, 512, 128), F32),
        pltpu.VMEM((512, 512), BF16),
        pltpu.VMEM((SEQS, COLS, WIDTH, 256), BF16),
        pltpu.VMEM((SEQS, COLS, WIDTH, 256), BF16),
        pltpu.VMEM((2, COLS * WIDTH, 128), F32),
        pltpu.VMEM((SEQS, 16 * ROWS, 256), BF16),
        pltpu.VMEM((SEQS, 16 * ROWS, 256), BF16),
        pltpu.VMEM((SEQS, TILE, D), F32),
        pltpu.VMEM((SEQS, TILE, D), BF16),
        dma((SEQS, TILES)), dma((10,)),
        pair, pair, pair, pair, pair, pair, pair, pair, pair,
        dma, dma, dma, dma,
    ]
    anywhere = pl.BlockSpec(memory_space=pl.ANY)
    return pl.pallas_call(
        kernel,
        out_shape=jax.ShapeDtypeStruct((SEQS, LOCAL, OUT), BF16),
        in_specs=[anywhere] * 11,
        out_specs=anywhere,
        scratch_shapes=scratch,
        compiler_params=pltpu.CompilerParams(
            collective_id=0, has_side_effects=True, vmem_limit_bytes=56 * 1024 * 1024
        ),
        name="fourier_mix",
    )(tokens, norm_gain.reshape(1, D), w_fourier_in, w_gate, w_spectrum, w_output, *tables())


def solution(mesh):
    placed = (P(None, "row", None), P(), P(None, "col"), P(), P(), P(None, "col"))
    return jax.shard_map(
        on_device, mesh=mesh, in_specs=placed, out_specs=P(None, "row", "col"), check_vma=False
    )
```

```python
import numpy as np
import jax
import jax.numpy as jnp
from jax import lax
from jax.experimental import pallas as pl
from jax.experimental.pallas import tpu as pltpu
from jax.sharding import PartitionSpec as P

MESH = pl.DeviceIdType.MESH
ROWS, COLS = 32, 8
SEQS, LOCAL, D = 2, 2048, 1024
TILE = 256
TILES = LOCAL // TILE
SEQ = ROWS * LOCAL
WIDTH = 64
CHANNELS = COLS * WIDTH
OUT = D // COLS
EPS = 1e-6
F32, BF16 = jnp.float32, jnp.bfloat16


def partner_channel(r, second):
    if r == 0:
        return 32 * second
    return WIDTH - r if second else r


def tables():
    n = np.arange(WIDTH)[:, None]
    analysis = np.zeros((2 * WIDTH, WIDTH))
    for r in range(ROWS):
        analysis[2 * r] = np.cos(2 * np.pi * n[:, 0] * r / WIDTH)
        analysis[2 * r + 1] = np.sin(2 * np.pi * n[:, 0] * r / WIDTH) if r else np.cos(np.pi * n[:, 0])
    a = np.arange(256)[:, None]
    p = np.arange(256)[None, :]
    turn = 2 * np.pi * (a * p % 256) / 256
    first = np.zeros((ROWS, 2, TILES, 4, 256))
    for e in range(2):
        first[:, e, :, 2 * e] = np.cos(turn).reshape(ROWS, TILES, 256)
        first[:, e, :, 2 * e + 1] = -np.sin(turn).reshape(ROWS, TILES, 256)
    first = first.reshape(2 * ROWS * TILES, 4 * 256)
    twist = 2 * np.pi * (a * p) / SEQ
    twist = np.concatenate([np.cos(twist), -np.sin(twist)], axis=1)
    second = np.concatenate([np.cos(turn), np.sin(turn)], axis=1) / np.sqrt(SEQ * WIDTH)
    select = np.zeros((CHANNELS, CHANNELS))
    for r in range(ROWS):
        for ch in range(2):
            for c in range(COLS):
                select[r * 16 + ch * 8 + c, c * WIDTH + partner_channel(r, ch)] = 1.0
    return (
        jnp.asarray(analysis, BF16),
        jnp.asarray(first, BF16),
        jnp.asarray(twist, F32),
        jnp.asarray(second, BF16),
        jnp.asarray(select, BF16),
    )


def dot(x, y, dims=((1,), (0,))):
    return lax.dot_general(x, y, (dims, ((), ())), preferred_element_type=F32)


def kernel(
    tokens, gain, w_in, w_gate, w_spec, w_out, analysis, first, twist, second, select,
    out,
    tok, gain_v, w_in_v, wc, w_gate_v, w_spec_v, w_map, w_out_v,
    analysis_v, first_v, twist_v, second_v, select_v,
    turned, send1, recv1, mid, both, sendx, recvx, wide, send2, recv2, sig, result,
    tok_sem, load_sem, s1, r1, sx, rx, s2, r2, so, ro, own_o, swo, rwo, swn, rwn, swy, rwy, sf, rf,
):
    row, col = lax.axis_index("row"), lax.axis_index("col")
    chip, core = col // 2, col % 2

    barrier = pltpu.get_barrier_semaphore()

    def greet_row(d, _):
        pl.semaphore_signal(barrier, inc=1, device_id=((row + d) % ROWS, col), device_id_type=MESH)
        return 0

    def greet_col(d, _):
        pl.semaphore_signal(barrier, inc=1, device_id=(row, (col + d) % COLS), device_id_type=MESH)
        return 0

    lax.fori_loop(1, ROWS, greet_row, 0)
    lax.fori_loop(1, COLS, greet_col, 0)

    def cols_of(c):
        return pl.ds(pl.multiple_of(c * OUT, OUT), OUT)

    loads = [
        pltpu.make_async_copy(src, dst, load_sem.at[i])
        for i, (src, dst) in enumerate(
            [
                (analysis, analysis_v), (w_in, w_in_v), (gain, gain_v),
                (first, first_v), (twist, twist_v), (second, second_v),
                (w_gate, w_gate_v), (w_out, w_out_v.at[:, cols_of(col)]),
                (w_spec, w_spec_v), (select, select_v),
            ]
        )
    ]

    def tile_copy(b, j):
        return pltpu.make_async_copy(
            tokens.at[b, pl.ds(pl.multiple_of(j * TILE, TILE), TILE)], tok.at[b, j], tok_sem.at[b, j]
        )

    for i in range(3):
        loads[i].start()
    for b in range(SEQS):
        for j in range(TILES):
            tile_copy(b, j).start()
    for i in range(3, 10):
        loads[i].start()

    for i in range(3):
        loads[i].wait()
    folded = dot(analysis_v[...], w_in_v[...]) * gain_v[...]
    wc[...] = jnp.transpose(folded).astype(BF16)

    def rows16(r):
        return pl.ds(pl.multiple_of(16 * r, 16), 16)

    def strided(ref, lo, hi, count, stride):
        halves = [
            jnp.concatenate([ref[h, pl.ds(at, count, stride), :] for at in (lo, hi)], axis=0) for h in range(2)
        ]
        return jnp.concatenate(halves, axis=1).astype(BF16)

    def project(b):
        def tile(j, _):
            tile_copy(b, j).wait()
            t = tok[b, j]
            wide_t = t.astype(F32)
            inverse = lax.rsqrt(jnp.sum(wide_t * wide_t, axis=1, keepdims=True) * (1.0 / D) + EPS)
            y = dot(t, wc[...]) * inverse
            flipped = jnp.transpose(y)[:WIDTH]
            for h in range(2):
                turned[h, pl.ds(pl.multiple_of(j * WIDTH, WIDTH), WIDTH), :] = flipped[:, 128 * h : 128 * (h + 1)]
            return 0

        lax.fori_loop(0, TILES, tile, 0)

        def pick(r, _):
            send1[b, rows16(r), :] = strided(turned, 2 * r, 2 * r + 1, TILES, WIDTH)
            return 0

        lax.fori_loop(0, ROWS, pick, 0)

    def row_send(src, dst, ssem, rsem, lanes):
        def one(i, _):
            k, l = i // 4, i % 4
            dz = 4 + (k + 1) // 2 * (1 - 2 * (k % 2))
            dy = 2 + (l + 1) // 2 * (1 - 2 * (l % 2))
            peer = (row // 4 + dz) % 8 * 4 + (row % 4 + dy) % 4
            pltpu.make_async_remote_copy(
                src_ref=src.at[rows16(peer), lanes], dst_ref=dst.at[rows16(row), lanes],
                send_sem=ssem, recv_sem=rsem, device_id=(peer, col), device_id_type=MESH,
            ).start()
            return 0

        lax.fori_loop(0, ROWS - 1, one, 0)
        dst[rows16(row), lanes] = src[rows16(row), lanes]

    def wait_bytes(ref, sem):
        pltpu.make_async_copy(ref, ref, sem).wait()

    most = pl.ds(0, 16 * (ROWS - 1))

    def col_send(b):
        def one(d, _):
            peer = (col + d) % COLS
            pltpu.make_async_remote_copy(
                src_ref=sendx.at[b, peer], dst_ref=recvx.at[b, col],
                send_sem=sx.at[b], recv_sem=rx.at[b], device_id=(row, peer), device_id_type=MESH,
            ).start()
            return 0

        lax.fori_loop(1, COLS, one, 0)
        recvx[b, col] = sendx[b, col]

    def fourier(b):
        y = dot(recv1[b], first_v[...], ((0,), (0,)))
        tr, ti = twist_v[:, :256], twist_v[:, 256:]
        ar, ai, br, bi = (y[:, 256 * i : 256 * (i + 1)] for i in range(4))
        pa, qa = ar * tr - ai * ti, ar * ti + ai * tr
        pb, qb = br * tr - bi * ti, br * ti + bi * tr
        lone = row == 0
        both[:256, :256] = pa.astype(BF16)
        both[256:, :256] = qa.astype(BF16)
        both[:256, 256:] = jnp.where(lone, pb, -qb).astype(BF16)
        both[256:, 256:] = jnp.where(lone, qb, pb).astype(BF16)
        d = dot(second_v[...], both[...])
        da, db = d[:, :256], d[:, 256:]
        made = (jnp.where(lone, da, da - db), jnp.where(lone, db, da + db))
        for ch in range(2):
            for h in range(2):
                mid[h, 256 * ch : 256 * (ch + 1)] = made[ch][:, 128 * h : 128 * (h + 1)]

        def pick(c, _):
            sendx[b, c] = strided(mid, c, 256 + c, ROWS, COLS)
            return 0

        lax.fori_loop(0, COLS, pick, 0)

    def regroup(b):
        def widen(c, _):
            block = recvx[b, c].astype(F32)
            for h in range(2):
                wide[h, pl.ds(pl.multiple_of(c * WIDTH, WIDTH), WIDTH), :] = block[:, 128 * h : 128 * (h + 1)]
            return 0

        lax.fori_loop(0, COLS, widen, 0)

        def pick(r, _):
            send2[b, rows16(r), :] = strided(wide, r, ROWS + r, COLS, WIDTH)
            return 0

        lax.fori_loop(0, ROWS, pick, 0)

    def gates(b):
        t = tok[b, col].astype(F32)
        inverse = lax.rsqrt(jnp.sum(t * t, axis=1, keepdims=True) * (1.0 / D) + EPS)
        normed = (t * inverse * gain_v[...]).astype(BF16)
        sig[b] = jax.nn.sigmoid(dot(normed, w_gate_v[...]))

    quarter = pl.ds(pl.multiple_of(row % 4 * 256, 256), 256)

    def shard_of(d):
        return cols_of((chip + d) % 4 * 2 + core)

    def share_out(rows, d, ssem, rsem, peer):
        return pltpu.make_async_remote_copy(
            src_ref=w_out_v.at[rows, shard_of(d)], dst_ref=w_out_v.at[rows, shard_of(d)],
            send_sem=ssem, recv_sem=rsem, device_id=peer, device_id_type=MESH,
        )

    def at_chip(d):
        return (row, (chip + d) % 4 * 2 + core)

    every = pl.ds(0, D)
    other_core = (row, chip * 2 + 1 - core)

    def finish(b, h):
        lanes = pl.ds(128 * h, 128)
        pre = dot(recv2[b, :, lanes], w_map[...], ((0,), (0,))).astype(BF16).astype(F32)
        mixed = (sig[b, lanes] * pre).astype(BF16)
        result[b, lanes] = dot(mixed, w_out_v[...]).astype(BF16)
        place = pl.ds(pl.multiple_of(col * TILE + 128 * h, 128), 128)

        def one(d, _):
            peer = (col + d) % COLS
            pltpu.make_async_remote_copy(
                src_ref=result.at[b, lanes, cols_of(peer)], dst_ref=out.at[b, place],
                send_sem=so.at[b, h], recv_sem=ro.at[b, h], device_id=(row, peer), device_id_type=MESH,
            ).start()
            return 0

        lax.fori_loop(1, COLS, one, 0)
        pltpu.make_async_copy(result.at[b, lanes, cols_of(col)], out.at[b, place], own_o.at[b, h]).start()

    whole = pl.ds(0, 256)

    def forward(b):
        row_send(send1.at[b], recv1.at[b], s1.at[b], r1.at[b], whole)

    def back(b):
        for h in range(2):
            row_send(send2.at[b], recv2.at[b], s2.at[b, h], r2.at[b, h], pl.ds(128 * h, 128))

    project(0)
    pl.semaphore_wait(barrier, ROWS - 1 + COLS - 1)
    forward(0)
    loads[7].wait()
    share_out(quarter, 0, swo, rwo, at_chip(2)).start()
    share_out(every, 0, swn, rwn, at_chip(1)).start()
    share_out(every, 0, swn, rwn, at_chip(3)).start()
    share_out(every, 0, sf, rf, other_core).start()
    project(1)
    wait_bytes(w_out_v.at[pl.ds(0, 256), pl.ds(0, OUT)], rwo)
    for d in range(1, 4):
        share_out(quarter, 2, swy, rwy, (row // 4 * 4 + (row % 4 + d) % 4, col)).start()
    loads[6].wait()
    gates(0)
    loads[8].wait()
    loads[9].wait()
    w_map[...] = dot(select_v[...], w_spec_v[...]).astype(BF16)
    for i in range(3, 6):
        loads[i].wait()

    wait_bytes(recv1.at[0, most], r1.at[0])
    forward(1)
    fourier(0)
    col_send(0)
    gates(1)
    wait_bytes(recvx.at[0, pl.ds(0, COLS - 1)], rx.at[0])
    regroup(0)
    back(0)
    wait_bytes(w_out_v.at[:, pl.ds(0, 2 * OUT)], rwn)
    wait_bytes(w_out_v.at[pl.ds(0, 768), pl.ds(0, OUT)], rwy)
    for d in range(1, 4):
        share_out(every, d, sf, rf, other_core).start()
    wait_bytes(recv1.at[1, most], r1.at[1])
    fourier(1)
    col_send(1)
    wait_bytes(recvx.at[1, pl.ds(0, COLS - 1)], rx.at[1])
    regroup(1)
    back(1)
    wait_bytes(w_out_v.at[:, pl.ds(0, 4 * OUT)], rf)
    for b in range(SEQS):
        for h in range(2):
            wait_bytes(recv2.at[b, most, pl.ds(128 * h, 128)], r2.at[b, h])
            finish(b, h)

    wait_bytes(w_out_v.at[pl.ds(0, 256), pl.ds(0, OUT)], swo)
    wait_bytes(w_out_v.at[:, pl.ds(0, 2 * OUT)], swn)
    wait_bytes(w_out_v.at[pl.ds(0, 768), pl.ds(0, OUT)], swy)
    wait_bytes(w_out_v.at[:, pl.ds(0, 4 * OUT)], sf)
    for b in range(SEQS):
        wait_bytes(send1.at[b, most], s1.at[b])
        wait_bytes(sendx.at[b, pl.ds(0, COLS - 1)], sx.at[b])
        for h in range(2):
            lanes = pl.ds(128 * h, 128)
            wait_bytes(send2.at[b, most, lanes], s2.at[b, h])
            wait_bytes(result.at[b, lanes, pl.ds(0, (COLS - 1) * OUT)], so.at[b, h])
            wait_bytes(out.at[b, pl.ds(0, (COLS - 1) * 128)], ro.at[b, h])
            wait_bytes(result.at[b, lanes, pl.ds(0, OUT)], own_o.at[b, h])


def on_device(tokens, norm_gain, w_fourier_in, w_gate, w_spectrum, w_output):
    dma = pltpu.SemaphoreType.DMA
    pair, halves = dma((SEQS,)), dma((SEQS, 2))
    scratch = [
        pltpu.VMEM((SEQS, TILES, TILE, D), BF16),
        pltpu.VMEM((1, D), F32),
        pltpu.VMEM((WIDTH, D), BF16),
        pltpu.VMEM((D, 2 * WIDTH), BF16),
        pltpu.VMEM((D, D), BF16),
        pltpu.VMEM((CHANNELS, D), BF16),
        pltpu.VMEM((CHANNELS, D), BF16),
        pltpu.VMEM((D, D), BF16),
        pltpu.VMEM((2 * WIDTH, WIDTH), BF16),
        pltpu.VMEM((512, 1024), BF16),
        pltpu.VMEM((256, 512), F32),
        pltpu.VMEM((256, 512), BF16),
        pltpu.VMEM((CHANNELS, CHANNELS), BF16),
        pltpu.VMEM((2, TILES * WIDTH, 128), F32),
        pltpu.VMEM((SEQS, 16 * ROWS, 256), BF16),
        pltpu.VMEM((SEQS, 16 * ROWS, 256), BF16),
        pltpu.VMEM((2, 512, 128), F32),
        pltpu.VMEM((512, 512), BF16),
        pltpu.VMEM((SEQS, COLS, WIDTH, 256), BF16),
        pltpu.VMEM((SEQS, COLS, WIDTH, 256), BF16),
        pltpu.VMEM((2, COLS * WIDTH, 128), F32),
        pltpu.VMEM((SEQS, 16 * ROWS, 256), BF16),
        pltpu.VMEM((SEQS, 16 * ROWS, 256), BF16),
        pltpu.VMEM((SEQS, TILE, D), F32),
        pltpu.VMEM((SEQS, TILE, D), BF16),
        dma((SEQS, TILES)), dma((10,)),
        pair, pair, pair, pair, halves, halves, halves, halves, halves,
        dma, dma, dma, dma, dma, dma, dma, dma,
    ]
    anywhere = pl.BlockSpec(memory_space=pl.ANY)
    return pl.pallas_call(
        kernel,
        out_shape=jax.ShapeDtypeStruct((SEQS, LOCAL, OUT), BF16),
        in_specs=[anywhere] * 11,
        out_specs=anywhere,
        scratch_shapes=scratch,
        compiler_params=pltpu.CompilerParams(
            collective_id=0, has_side_effects=True, vmem_limit_bytes=56 * 1024 * 1024
        ),
        name="fourier_mix",
    )(tokens, norm_gain.reshape(1, D), w_fourier_in.T, w_gate, w_spectrum, w_output, *tables())


def solution(mesh):
    placed = (P(None, "row", None), P(), P(None, "col"), P(), P(), P(None, "col"))
    return jax.shard_map(
        on_device, mesh=mesh, in_specs=placed, out_specs=P(None, "row", "col"), check_vma=False
    )
```

```python
import numpy as np
import jax
import jax.numpy as jnp
from jax import lax
from jax.experimental import pallas as pl
from jax.experimental.pallas import tpu as pltpu
from jax.sharding import PartitionSpec as P

MESH = pl.DeviceIdType.MESH
ROWS, COLS = 32, 8
SEQS, LOCAL, D = 2, 2048, 1024
TILE = 256
TILES = LOCAL // TILE
SEQ = ROWS * LOCAL
WIDTH = 64
CHANNELS = COLS * WIDTH
OUT = D // COLS
EPS = 1e-6
F32, BF16 = jnp.float32, jnp.bfloat16


def partner_channel(r, second):
    if r == 0:
        return 32 * second
    return WIDTH - r if second else r


def tables():
    n = np.arange(WIDTH)[:, None]
    analysis = np.zeros((2 * WIDTH, WIDTH))
    for r in range(ROWS):
        analysis[2 * r] = np.cos(2 * np.pi * n[:, 0] * r / WIDTH)
        analysis[2 * r + 1] = np.sin(2 * np.pi * n[:, 0] * r / WIDTH) if r else np.cos(np.pi * n[:, 0])
    a = np.arange(256)[:, None]
    p = np.arange(256)[None, :]
    turn = 2 * np.pi * (a * p % 256) / 256
    first = np.zeros((ROWS, 2, TILES, 4, 256))
    for e in range(2):
        first[:, e, :, 2 * e] = np.cos(turn).reshape(ROWS, TILES, 256)
        first[:, e, :, 2 * e + 1] = -np.sin(turn).reshape(ROWS, TILES, 256)
    first = first.reshape(2 * ROWS * TILES, 4, 2, 128).transpose(2, 0, 1, 3).reshape(2, 2 * ROWS * TILES, 512)
    twist = 2 * np.pi * (a * p) / SEQ
    twist = np.stack([np.cos(twist), -np.sin(twist)], axis=1).reshape(256, 2, 2, 128)
    twist = twist.transpose(2, 0, 1, 3).reshape(2, 256, 256)
    second = np.concatenate([np.cos(turn), np.sin(turn)], axis=1) / np.sqrt(SEQ * WIDTH)
    select = np.zeros((CHANNELS, CHANNELS))
    for r in range(ROWS):
        for ch in range(2):
            for c in range(COLS):
                select[r * 16 + ch * 8 + c, c * WIDTH + partner_channel(r, ch)] = 1.0
    return (
        jnp.asarray(analysis, BF16),
        jnp.asarray(first, BF16),
        jnp.asarray(twist, F32),
        jnp.asarray(second, BF16),
        jnp.asarray(select, BF16),
    )


def dot(x, y, dims=((1,), (0,))):
    return lax.dot_general(x, y, (dims, ((), ())), preferred_element_type=F32)


def kernel(
    tokens, gain, w_in, w_gate, w_spec, w_out, analysis, first, twist, second, select,
    out,
    tok, gain_v, w_in_v, wc, w_gate_v, w_spec_v, w_map, w_out_v,
    analysis_v, first_v, twist_v, second_v, select_v,
    turned, send1, recv1, mid, both, sendx, recvx, wide, send2, recv2, sig, result,
    tok_sem, load_sem, s1, r1, sx, rx, s2, r2, so, ro, own_o, swo, rwo, swn, rwn, swy, rwy, sf, rf,
):
    row, col = lax.axis_index("row"), lax.axis_index("col")
    chip, core = col // 2, col % 2

    barrier = pltpu.get_barrier_semaphore()

    def greet_row(d, _):
        pl.semaphore_signal(barrier, inc=1, device_id=((row + d) % ROWS, col), device_id_type=MESH)
        return 0

    def greet_col(d, _):
        pl.semaphore_signal(barrier, inc=1, device_id=(row, (col + d) % COLS), device_id_type=MESH)
        return 0

    lax.fori_loop(1, ROWS, greet_row, 0)
    lax.fori_loop(1, COLS, greet_col, 0)

    def cols_of(c):
        return pl.ds(pl.multiple_of(c * OUT, OUT), OUT)

    loads = [
        pltpu.make_async_copy(src, dst, load_sem.at[i])
        for i, (src, dst) in enumerate(
            [
                (analysis, analysis_v), (w_in, w_in_v), (gain, gain_v),
                (first, first_v), (twist, twist_v), (second, second_v),
                (w_gate, w_gate_v), (w_out, w_out_v.at[:, cols_of(col)]),
                (w_spec, w_spec_v), (select, select_v),
            ]
        )
    ]

    def tile_copy(b, j):
        return pltpu.make_async_copy(
            tokens.at[b, pl.ds(pl.multiple_of(j * TILE, TILE), TILE)], tok.at[b, j], tok_sem.at[b, j]
        )

    for i in range(3):
        loads[i].start()
    for b in range(SEQS):
        for j in range(TILES):
            tile_copy(b, j).start()
    for i in range(3, 10):
        loads[i].start()

    for i in range(3):
        loads[i].wait()
    folded = dot(analysis_v[...], w_in_v[...]) * gain_v[...]
    wc[...] = jnp.transpose(folded).astype(BF16)

    def rows16(r):
        return pl.ds(pl.multiple_of(16 * r, 16), 16)

    def strided(ref, h, lo, hi, count, stride):
        rows = [ref[h, pl.ds(at, count, stride), :] for at in (lo, hi)]
        return jnp.concatenate(rows, axis=0).astype(BF16)

    def project(b):
        def tile(j, _):
            tile_copy(b, j).wait()
            t = tok[b, j]
            wide_t = t.astype(F32)
            inverse = lax.rsqrt(jnp.sum(wide_t * wide_t, axis=1, keepdims=True) * (1.0 / D) + EPS)
            y = dot(t, wc[...]) * inverse
            flipped = jnp.transpose(y)[:WIDTH]
            for h in range(2):
                turned[h, pl.ds(pl.multiple_of(j * WIDTH, WIDTH), WIDTH), :] = flipped[:, 128 * h : 128 * (h + 1)]
            return 0

        lax.fori_loop(0, TILES, tile, 0)

        def pick(i, _):
            for u in range(4):
                r = 4 * i + u
                for h in range(2):
                    lanes = slice(128 * h, 128 * (h + 1))
                    send1[b, rows16(r), lanes] = strided(turned, h, 2 * r, 2 * r + 1, TILES, WIDTH)
            return 0

        lax.fori_loop(0, ROWS // 4, pick, 0)

    peers_z = [((row // 4 + dz) % 8) * 4 for dz in range(8)]
    peers_y = [(row % 4 + dy) % 4 for dy in range(4)]
    far_first = sorted(
        ((dz, dy) for dz in range(8) for dy in range(4) if dz or dy),
        key=lambda o: -(min(o[0], 8 - o[0]) + min(o[1], 4 - o[1])),
    )

    def row_send(src, dst, ssem, rsem):
        mine = rows16(row)
        for dz, dy in far_first:
            peer = peers_z[dz] + peers_y[dy]
            pltpu.make_async_remote_copy(
                src_ref=src.at[rows16(peer)], dst_ref=dst.at[mine],
                send_sem=ssem, recv_sem=rsem, device_id=(peer, col), device_id_type=MESH,
            ).start()
        dst[mine, :] = src[mine, :]

    def wait_bytes(ref, sem):
        pltpu.make_async_copy(ref, ref, sem).wait()

    most = pl.ds(0, 16 * (ROWS - 1))
    peers_c = [(col + d) % COLS for d in range(COLS)]
    col_order = (4, 5, 3, 2, 6, 7, 1)

    def col_send(b, h):
        for d in col_order:
            peer = peers_c[d]
            pltpu.make_async_remote_copy(
                src_ref=sendx.at[b, h, peer], dst_ref=recvx.at[b, h, col],
                send_sem=sx.at[b, h], recv_sem=rx.at[b, h], device_id=(row, peer), device_id_type=MESH,
            ).start()
        recvx[b, h, col] = sendx[b, h, col]

    def fourier(b):
        lone = row == 0
        across = jnp.transpose(recv1[b])
        for h in range(2):
            y = dot(across, first_v[h])
            tr, ti = twist_v[h, :, :128], twist_v[h, :, 128:]
            ar, ai, br, bi = (y[:, 128 * i : 128 * (i + 1)] for i in range(4))
            pa, qa = ar * tr - ai * ti, ar * ti + ai * tr
            pb, qb = br * tr - bi * ti, br * ti + bi * tr
            both[h, :256, :128] = pa.astype(BF16)
            both[h, 256:, :128] = qa.astype(BF16)
            both[h, :256, 128:] = jnp.where(lone, pb, -qb).astype(BF16)
            both[h, 256:, 128:] = jnp.where(lone, qb, pb).astype(BF16)
            d = dot(second_v[...], both[h])
            da, db = d[:, :128], d[:, 128:]
            mid[h, :256] = jnp.where(lone, da, da - db)
            mid[h, 256:] = jnp.where(lone, db, da + db)
            for c in range(COLS):
                sendx[b, h, c] = strided(mid, h, c, 256 + c, ROWS, COLS)
            col_send(b, h)

    def regroup(b, h):
        for c in range(COLS):
            wide[h, c * WIDTH : (c + 1) * WIDTH, :] = recvx[b, h, c].astype(F32)

        def pick(i, _):
            for u in range(4):
                r = 4 * i + u
                send2[b, h, rows16(r), :] = strided(wide, h, r, ROWS + r, COLS, WIDTH)
            return 0

        lax.fori_loop(0, ROWS // 4, pick, 0)

    def gates(b):
        t = tok[b, col].astype(F32)
        inverse = lax.rsqrt(jnp.sum(t * t, axis=1, keepdims=True) * (1.0 / D) + EPS)
        normed = (t * inverse * gain_v[...]).astype(BF16)
        sig[b] = jax.nn.sigmoid(dot(normed, w_gate_v[...]))

    quarter = pl.ds(pl.multiple_of(row % 4 * 256, 256), 256)

    def shard_of(d):
        return cols_of((chip + d) % 4 * 2 + core)

    def share_out(rows, d, ssem, rsem, peer):
        return pltpu.make_async_remote_copy(
            src_ref=w_out_v.at[rows, shard_of(d)], dst_ref=w_out_v.at[rows, shard_of(d)],
            send_sem=ssem, recv_sem=rsem, device_id=peer, device_id_type=MESH,
        )

    def at_chip(d):
        return (row, (chip + d) % 4 * 2 + core)

    every = pl.ds(0, D)
    other_core = (row, chip * 2 + 1 - core)

    def finish(b, h):
        lanes = pl.ds(128 * h, 128)
        pre = dot(recv2[b, h], w_map[...], ((0,), (0,))).astype(BF16).astype(F32)
        mixed = (sig[b, lanes] * pre).astype(BF16)
        result[b, lanes] = dot(mixed, w_out_v[...]).astype(BF16)
        place = pl.ds(pl.multiple_of(col * TILE + 128 * h, 128), 128)

        for d in col_order:
            peer = peers_c[d]
            pltpu.make_async_remote_copy(
                src_ref=result.at[b, lanes, cols_of(peer)], dst_ref=out.at[b, place],
                send_sem=so.at[b, h], recv_sem=ro.at[b, h], device_id=(row, peer), device_id_type=MESH,
            ).start()
        pltpu.make_async_copy(result.at[b, lanes, cols_of(col)], out.at[b, place], own_o.at[b, h]).start()

    def forward(b):
        row_send(send1.at[b], recv1.at[b], s1.at[b], r1.at[b])

    def back(b, h):
        wait_bytes(recvx.at[b, h, pl.ds(0, COLS - 1)], rx.at[b, h])
        regroup(b, h)
        row_send(send2.at[b, h], recv2.at[b, h], s2.at[b, h], r2.at[b, h])

    project(0)
    pl.semaphore_wait(barrier, ROWS - 1 + COLS - 1)
    forward(0)
    loads[7].wait()
    share_out(quarter, 0, swo, rwo, at_chip(2)).start()
    share_out(every, 0, swn, rwn, at_chip(1)).start()
    share_out(every, 0, swn, rwn, at_chip(3)).start()
    share_out(every, 0, sf, rf, other_core).start()
    project(1)
    loads[6].wait()
    gates(0)
    loads[8].wait()
    loads[9].wait()
    w_map[...] = dot(select_v[...], w_spec_v[...]).astype(BF16)
    forward(1)
    gates(1)
    wait_bytes(w_out_v.at[pl.ds(0, 256), pl.ds(0, OUT)], rwo)
    for d in range(1, 4):
        share_out(quarter, 2, swy, rwy, (row // 4 * 4 + (row % 4 + d) % 4, col)).start()
    for i in range(3, 6):
        loads[i].wait()

    wait_bytes(recv1.at[0, most], r1.at[0])
    fourier(0)
    back(0, 0)
    back(0, 1)
    wait_bytes(recv1.at[1, most], r1.at[1])
    fourier(1)
    wait_bytes(w_out_v.at[:, pl.ds(0, 2 * OUT)], rwn)
    wait_bytes(w_out_v.at[pl.ds(0, 768), pl.ds(0, OUT)], rwy)
    for d in range(1, 4):
        share_out(every, d, sf, rf, other_core).start()
    back(1, 0)
    back(1, 1)
    wait_bytes(w_out_v.at[:, pl.ds(0, 4 * OUT)], rf)
    for b in range(SEQS):
        for h in range(2):
            wait_bytes(recv2.at[b, h, most], r2.at[b, h])
            finish(b, h)

    wait_bytes(w_out_v.at[pl.ds(0, 256), pl.ds(0, OUT)], swo)
    wait_bytes(w_out_v.at[:, pl.ds(0, 2 * OUT)], swn)
    wait_bytes(w_out_v.at[pl.ds(0, 768), pl.ds(0, OUT)], swy)
    wait_bytes(w_out_v.at[:, pl.ds(0, 4 * OUT)], sf)
    for b in range(SEQS):
        wait_bytes(send1.at[b, most], s1.at[b])
        for h in range(2):
            lanes = pl.ds(128 * h, 128)
            wait_bytes(sendx.at[b, h, pl.ds(0, COLS - 1)], sx.at[b, h])
            wait_bytes(send2.at[b, h, most], s2.at[b, h])
            wait_bytes(result.at[b, lanes, pl.ds(0, (COLS - 1) * OUT)], so.at[b, h])
            wait_bytes(out.at[b, pl.ds(0, (COLS - 1) * 128)], ro.at[b, h])
            wait_bytes(result.at[b, lanes, pl.ds(0, OUT)], own_o.at[b, h])


def on_device(tokens, norm_gain, w_fourier_in, w_gate, w_spectrum, w_output):
    dma = pltpu.SemaphoreType.DMA
    pair, halves = dma((SEQS,)), dma((SEQS, 2))
    scratch = [
        pltpu.VMEM((SEQS, TILES, TILE, D), BF16),
        pltpu.VMEM((1, D), F32),
        pltpu.VMEM((WIDTH, D), BF16),
        pltpu.VMEM((D, 2 * WIDTH), BF16),
        pltpu.VMEM((D, D), BF16),
        pltpu.VMEM((CHANNELS, D), BF16),
        pltpu.VMEM((CHANNELS, D), BF16),
        pltpu.VMEM((D, D), BF16),
        pltpu.VMEM((2 * WIDTH, WIDTH), BF16),
        pltpu.VMEM((2, 512, 512), BF16),
        pltpu.VMEM((2, 256, 256), F32),
        pltpu.VMEM((256, 512), BF16),
        pltpu.VMEM((CHANNELS, CHANNELS), BF16),
        pltpu.VMEM((2, TILES * WIDTH, 128), F32),
        pltpu.VMEM((SEQS, 16 * ROWS, 256), BF16),
        pltpu.VMEM((SEQS, 16 * ROWS, 256), BF16),
        pltpu.VMEM((2, 512, 128), F32),
        pltpu.VMEM((2, 512, 256), BF16),
        pltpu.VMEM((SEQS, 2, COLS, WIDTH, 128), BF16),
        pltpu.VMEM((SEQS, 2, COLS, WIDTH, 128), BF16),
        pltpu.VMEM((2, COLS * WIDTH, 128), F32),
        pltpu.VMEM((SEQS, 2, 16 * ROWS, 128), BF16),
        pltpu.VMEM((SEQS, 2, 16 * ROWS, 128), BF16),
        pltpu.VMEM((SEQS, TILE, D), F32),
        pltpu.VMEM((SEQS, TILE, D), BF16),
        dma((SEQS, TILES)), dma((10,)),
        pair, pair, halves, halves, halves, halves, halves, halves, halves,
        dma, dma, dma, dma, dma, dma, dma, dma,
    ]
    anywhere = pl.BlockSpec(memory_space=pl.ANY)
    return pl.pallas_call(
        kernel,
        out_shape=jax.ShapeDtypeStruct((SEQS, LOCAL, OUT), BF16),
        in_specs=[anywhere] * 11,
        out_specs=anywhere,
        scratch_shapes=scratch,
        compiler_params=pltpu.CompilerParams(
            collective_id=0, has_side_effects=True, vmem_limit_bytes=56 * 1024 * 1024
        ),
        name="fourier_mix",
    )(tokens, norm_gain.reshape(1, D), w_fourier_in.T, w_gate, w_spectrum, w_output, *tables())


def solution(mesh):
    placed = (P(None, "row", None), P(), P(None, "col"), P(), P(), P(None, "col"))
    return jax.shard_map(
        on_device, mesh=mesh, in_specs=placed, out_specs=P(None, "row", "col"), check_vma=False
    )
```

```python
import numpy as np
import jax
import jax.numpy as jnp
from jax import lax
from jax.experimental import pallas as pl
from jax.experimental.pallas import tpu as pltpu
from jax.sharding import PartitionSpec as P

MESH = pl.DeviceIdType.MESH
ROWS, COLS = 32, 8
SEQS, LOCAL, D = 2, 2048, 1024
TILE = 256
TILES = LOCAL // TILE
SEQ = ROWS * LOCAL
WIDTH = 64
CHANNELS = COLS * WIDTH
OUT = D // COLS
EPS = 1e-6
F32, BF16 = jnp.float32, jnp.bfloat16


def partner_channel(r, second):
    if r == 0:
        return 32 * second
    return WIDTH - r if second else r


def tables():
    n = np.arange(WIDTH)[:, None]
    analysis = np.zeros((2 * WIDTH, WIDTH))
    for r in range(ROWS):
        analysis[2 * r] = np.cos(2 * np.pi * n[:, 0] * r / WIDTH)
        analysis[2 * r + 1] = np.sin(2 * np.pi * n[:, 0] * r / WIDTH) if r else np.cos(np.pi * n[:, 0])
    a = np.arange(256)[:, None]
    p = np.arange(256)[None, :]
    turn = 2 * np.pi * (a * p % 256) / 256
    first = np.zeros((ROWS, 2, TILES, 4, 256))
    for e in range(2):
        first[:, e, :, 2 * e] = np.cos(turn).reshape(ROWS, TILES, 256)
        first[:, e, :, 2 * e + 1] = -np.sin(turn).reshape(ROWS, TILES, 256)
    first = first.reshape(2 * ROWS * TILES, 4, 2, 128).transpose(2, 0, 1, 3).reshape(2, 2 * ROWS * TILES, 512)
    twist = 2 * np.pi * (a * p) / SEQ
    twist = np.stack([np.cos(twist), -np.sin(twist)], axis=1).reshape(256, 2, 2, 128)
    twist = twist.transpose(2, 0, 1, 3).reshape(2, 256, 256)
    second = np.concatenate([np.cos(turn), np.sin(turn)], axis=1) / np.sqrt(SEQ * WIDTH)
    select = np.zeros((CHANNELS, CHANNELS))
    for r in range(ROWS):
        for ch in range(2):
            for c in range(COLS):
                select[r * 16 + ch * 8 + c, c * WIDTH + partner_channel(r, ch)] = 1.0
    return (
        jnp.asarray(analysis, BF16),
        jnp.asarray(first, BF16),
        jnp.asarray(twist, F32),
        jnp.asarray(second, BF16),
        jnp.asarray(select, BF16),
    )


def dot(x, y, dims=((1,), (0,))):
    return lax.dot_general(x, y, (dims, ((), ())), preferred_element_type=F32)


def kernel(
    tokens, gain, w_in, w_gate, w_spec, w_out, analysis, first, twist, second, select,
    out,
    tok, gain_v, w_in_v, wc, w_gate_v, w_spec_v, w_map, w_out_v,
    analysis_v, first_v, twist_v, second_v, select_v,
    turned, send1, recv1, mid, both, sendx, recvx, wide, send2, recv2, sig, result,
    tok_sem, load_sem, s1, r1, sx, rx, s2, r2, so, ro, own_o, swo, rwo, swn, rwn, swy, rwy, sf, rf,
):
    row, col = lax.axis_index("row"), lax.axis_index("col")
    chip, core = col // 2, col % 2

    barrier = pltpu.get_barrier_semaphore()

    def greet_row(d, _):
        pl.semaphore_signal(barrier, inc=1, device_id=((row + d) % ROWS, col), device_id_type=MESH)
        return 0

    def greet_col(d, _):
        pl.semaphore_signal(barrier, inc=1, device_id=(row, (col + d) % COLS), device_id_type=MESH)
        return 0

    lax.fori_loop(1, ROWS, greet_row, 0)
    lax.fori_loop(1, COLS, greet_col, 0)

    def cols_of(c):
        return pl.ds(pl.multiple_of(c * OUT, OUT), OUT)

    loads = [
        pltpu.make_async_copy(src, dst, load_sem.at[i])
        for i, (src, dst) in enumerate(
            [
                (analysis, analysis_v), (w_in, w_in_v), (gain, gain_v),
                (first, first_v), (twist, twist_v), (second, second_v),
                (w_gate, w_gate_v), (w_out, w_out_v.at[:, cols_of(col)]),
                (w_spec, w_spec_v), (select, select_v),
            ]
        )
    ]

    def tile_copy(b, j):
        return pltpu.make_async_copy(
            tokens.at[b, pl.ds(pl.multiple_of(j * TILE, TILE), TILE)], tok.at[b, j], tok_sem.at[b, j]
        )

    for i in range(3):
        loads[i].start()
    for b in range(SEQS):
        for j in range(TILES):
            tile_copy(b, j).start()
    for i in range(3, 10):
        loads[i].start()

    for i in range(3):
        loads[i].wait()
    folded = dot(analysis_v[...], w_in_v[...]) * gain_v[...]
    wc[...] = jnp.transpose(folded).astype(BF16)

    def rows16(r):
        return pl.ds(pl.multiple_of(16 * r, 16), 16)

    def strided(ref, h, lo, hi, count, stride):
        rows = [ref[h, pl.ds(at, count, stride), :] for at in (lo, hi)]
        return jnp.concatenate(rows, axis=0).astype(BF16)

    def project(b):
        def tile(j, _):
            tile_copy(b, j).wait()
            t = tok[b, j]
            wide_t = t.astype(F32)
            inverse = lax.rsqrt(jnp.sum(wide_t * wide_t, axis=1, keepdims=True) * (1.0 / D) + EPS)
            y = dot(t, wc[...]) * inverse
            flipped = jnp.transpose(y)[:WIDTH]
            for h in range(2):
                turned[h, pl.ds(pl.multiple_of(j * WIDTH, WIDTH), WIDTH), :] = flipped[:, 128 * h : 128 * (h + 1)]
            return 0

        lax.fori_loop(0, TILES, tile, 0)

        def pick(i, _):
            for u in range(4):
                r = 4 * i + u
                for h in range(2):
                    lanes = slice(128 * h, 128 * (h + 1))
                    send1[b, rows16(r), lanes] = strided(turned, h, 2 * r, 2 * r + 1, TILES, WIDTH)
            return 0

        lax.fori_loop(0, ROWS // 4, pick, 0)

    peers_z = [((row // 4 + dz) % 8) * 4 for dz in range(8)]
    peers_y = [(row % 4 + dy) % 4 for dy in range(4)]
    far_first = sorted(
        ((dz, dy) for dz in range(8) for dy in range(4) if dz or dy),
        key=lambda o: -(min(o[0], 8 - o[0]) + min(o[1], 4 - o[1])),
    )

    def row_send(src, dst, ssem, rsem):
        mine = rows16(row)
        for dz, dy in far_first:
            peer = peers_z[dz] + peers_y[dy]
            pltpu.make_async_remote_copy(
                src_ref=src.at[rows16(peer)], dst_ref=dst.at[mine],
                send_sem=ssem, recv_sem=rsem, device_id=(peer, col), device_id_type=MESH,
            ).start()
        dst[mine, :] = src[mine, :]

    def wait_bytes(ref, sem):
        pltpu.make_async_copy(ref, ref, sem).wait()

    most = pl.ds(0, 16 * (ROWS - 1))
    peers_c = [(col + d) % COLS for d in range(COLS)]
    col_order = (4, 5, 3, 2, 6, 7, 1)

    def col_send(b, h):
        for d in col_order:
            peer = peers_c[d]
            pltpu.make_async_remote_copy(
                src_ref=sendx.at[b, h, peer], dst_ref=recvx.at[b, h, col],
                send_sem=sx.at[b, h], recv_sem=rx.at[b, h], device_id=(row, peer), device_id_type=MESH,
            ).start()
        recvx[b, h, col] = sendx[b, h, col]

    def fourier(b):
        lone = row == 0
        across = jnp.transpose(recv1[b])
        for h in range(2):
            y = dot(across, first_v[h])
            tr, ti = twist_v[h, :, :128], twist_v[h, :, 128:]
            ar, ai, br, bi = (y[:, 128 * i : 128 * (i + 1)] for i in range(4))
            pa, qa = ar * tr - ai * ti, ar * ti + ai * tr
            pb, qb = br * tr - bi * ti, br * ti + bi * tr
            both[h, :256, :128] = pa.astype(BF16)
            both[h, 256:, :128] = qa.astype(BF16)
            both[h, :256, 128:] = jnp.where(lone, pb, -qb).astype(BF16)
            both[h, 256:, 128:] = jnp.where(lone, qb, pb).astype(BF16)
            d = dot(second_v[...], both[h])
            da, db = d[:, :128], d[:, 128:]
            mid[h, :256] = jnp.where(lone, da, da - db)
            mid[h, 256:] = jnp.where(lone, db, da + db)
            for c in range(COLS):
                sendx[b, h, c] = strided(mid, h, c, 256 + c, ROWS, COLS)
            col_send(b, h)

    def regroup(b, h):
        for c in range(COLS):
            wide[h, c * WIDTH : (c + 1) * WIDTH, :] = recvx[b, h, c].astype(F32)

        def pick(i, _):
            for u in range(4):
                r = 4 * i + u
                send2[b, h, rows16(r), :] = strided(wide, h, r, ROWS + r, COLS, WIDTH)
            return 0

        lax.fori_loop(0, ROWS // 4, pick, 0)

    def gates(b):
        t = tok[b, col].astype(F32)
        inverse = lax.rsqrt(jnp.sum(t * t, axis=1, keepdims=True) * (1.0 / D) + EPS)
        normed = (t * inverse * gain_v[...]).astype(BF16)
        sig[b] = jax.nn.sigmoid(dot(normed, w_gate_v[...]))

    quarter = pl.ds(pl.multiple_of(row % 4 * 256, 256), 256)

    def shard_of(d):
        return cols_of((chip + d) % 4 * 2 + core)

    def share_out(rows, d, ssem, rsem, peer):
        return pltpu.make_async_remote_copy(
            src_ref=w_out_v.at[rows, shard_of(d)], dst_ref=w_out_v.at[rows, shard_of(d)],
            send_sem=ssem, recv_sem=rsem, device_id=peer, device_id_type=MESH,
        )

    def at_chip(d):
        return (row, (chip + d) % 4 * 2 + core)

    every = pl.ds(0, D)
    other_core = (row, chip * 2 + 1 - core)

    def finish(b, h):
        lanes = pl.ds(128 * h, 128)
        pre = dot(recv2[b, h], w_map[...], ((0,), (0,))).astype(BF16).astype(F32)
        mixed = (sig[b, lanes] * pre).astype(BF16)
        result[b, lanes] = dot(mixed, w_out_v[...]).astype(BF16)
        place = pl.ds(pl.multiple_of(col * TILE + 128 * h, 128), 128)

        for d in col_order:
            peer = peers_c[d]
            pltpu.make_async_remote_copy(
                src_ref=result.at[b, lanes, cols_of(peer)], dst_ref=out.at[b, place],
                send_sem=so.at[b, h], recv_sem=ro.at[b, h], device_id=(row, peer), device_id_type=MESH,
            ).start()
        pltpu.make_async_copy(result.at[b, lanes, cols_of(col)], out.at[b, place], own_o.at[b, h]).start()

    def forward(b):
        row_send(send1.at[b], recv1.at[b], s1.at[b], r1.at[b])

    def back(b, h):
        wait_bytes(recvx.at[b, h, pl.ds(0, COLS - 1)], rx.at[b, h])
        regroup(b, h)
        row_send(send2.at[b, h], recv2.at[b, h], s2.at[b, h], r2.at[b, h])

    project(0)
    pl.semaphore_wait(barrier, ROWS - 1 + COLS - 1)
    forward(0)
    loads[7].wait()
    share_out(quarter, 0, swo, rwo, at_chip(2)).start()
    share_out(every, 0, swn, rwn, at_chip(1)).start()
    share_out(every, 0, swn, rwn, at_chip(3)).start()
    share_out(every, 0, sf, rf, other_core).start()
    project(1)
    loads[6].wait()
    gates(0)
    loads[8].wait()
    loads[9].wait()
    w_map[...] = dot(select_v[...], w_spec_v[...]).astype(BF16)
    forward(1)
    gates(1)
    wait_bytes(w_out_v.at[pl.ds(0, 256), pl.ds(0, OUT)], rwo)
    for d in range(1, 4):
        share_out(quarter, 2, swy, rwy, (row // 4 * 4 + (row % 4 + d) % 4, col)).start()
    for i in range(3, 6):
        loads[i].wait()

    wait_bytes(recv1.at[0, most], r1.at[0])
    fourier(0)
    back(0, 0)
    back(0, 1)
    wait_bytes(recv1.at[1, most], r1.at[1])
    fourier(1)
    wait_bytes(w_out_v.at[:, pl.ds(0, 2 * OUT)], rwn)
    wait_bytes(w_out_v.at[pl.ds(0, 768), pl.ds(0, OUT)], rwy)
    for d in range(1, 4):
        share_out(every, d, sf, rf, other_core).start()
    back(1, 0)
    back(1, 1)
    wait_bytes(w_out_v.at[:, pl.ds(0, 4 * OUT)], rf)
    for b in range(SEQS):
        for h in range(2):
            wait_bytes(recv2.at[b, h, most], r2.at[b, h])
            finish(b, h)

    wait_bytes(w_out_v.at[pl.ds(0, 256), pl.ds(0, OUT)], swo)
    wait_bytes(w_out_v.at[:, pl.ds(0, 2 * OUT)], swn)
    wait_bytes(w_out_v.at[pl.ds(0, 768), pl.ds(0, OUT)], swy)
    wait_bytes(w_out_v.at[:, pl.ds(0, 4 * OUT)], sf)
    for b in range(SEQS):
        wait_bytes(send1.at[b, most], s1.at[b])
        for h in range(2):
            lanes = pl.ds(128 * h, 128)
            wait_bytes(sendx.at[b, h, pl.ds(0, COLS - 1)], sx.at[b, h])
            wait_bytes(send2.at[b, h, most], s2.at[b, h])
            wait_bytes(result.at[b, lanes, pl.ds(0, (COLS - 1) * OUT)], so.at[b, h])
            wait_bytes(out.at[b, pl.ds(0, (COLS - 1) * 128)], ro.at[b, h])
            wait_bytes(result.at[b, lanes, pl.ds(0, OUT)], own_o.at[b, h])


def on_device(tokens, norm_gain, w_fourier_in, w_gate, w_spectrum, w_output):
    dma = pltpu.SemaphoreType.DMA
    pair, halves = dma((SEQS,)), dma((SEQS, 2))
    scratch = [
        pltpu.VMEM((SEQS, TILES, TILE, D), BF16),
        pltpu.VMEM((1, D), F32),
        pltpu.VMEM((WIDTH, D), BF16),
        pltpu.VMEM((D, 2 * WIDTH), BF16),
        pltpu.VMEM((D, D), BF16),
        pltpu.VMEM((CHANNELS, D), BF16),
        pltpu.VMEM((CHANNELS, D), BF16),
        pltpu.VMEM((D, D), BF16),
        pltpu.VMEM((2 * WIDTH, WIDTH), BF16),
        pltpu.VMEM((2, 512, 512), BF16),
        pltpu.VMEM((2, 256, 256), F32),
        pltpu.VMEM((256, 512), BF16),
        pltpu.VMEM((CHANNELS, CHANNELS), BF16),
        pltpu.VMEM((2, TILES * WIDTH, 128), F32),
        pltpu.VMEM((SEQS, 16 * ROWS, 256), BF16),
        pltpu.VMEM((SEQS, 16 * ROWS, 256), BF16),
        pltpu.VMEM((2, 512, 128), F32),
        pltpu.VMEM((2, 512, 256), BF16),
        pltpu.VMEM((SEQS, 2, COLS, WIDTH, 128), BF16),
        pltpu.VMEM((SEQS, 2, COLS, WIDTH, 128), BF16),
        pltpu.VMEM((2, COLS * WIDTH, 128), F32),
        pltpu.VMEM((SEQS, 2, 16 * ROWS, 128), BF16),
        pltpu.VMEM((SEQS, 2, 16 * ROWS, 128), BF16),
        pltpu.VMEM((SEQS, TILE, D), F32),
        pltpu.VMEM((SEQS, TILE, D), BF16),
        dma((SEQS, TILES)), dma((10,)),
        pair, pair, halves, halves, halves, halves, halves, halves, halves,
        dma, dma, dma, dma, dma, dma, dma, dma,
    ]
    anywhere = pl.BlockSpec(memory_space=pl.ANY)
    return pl.pallas_call(
        kernel,
        out_shape=pltpu.VMEM((SEQS, LOCAL, OUT), BF16),
        in_specs=[anywhere] * 11,
        out_specs=anywhere,
        scratch_shapes=scratch,
        compiler_params=pltpu.CompilerParams(
            collective_id=0, has_side_effects=True, vmem_limit_bytes=56 * 1024 * 1024
        ),
        name="fourier_mix",
    )(tokens, norm_gain.reshape(1, D), w_fourier_in.T, w_gate, w_spectrum, w_output, *tables())


def solution(mesh):
    placed = (P(None, "row", None), P(), P(None, "col"), P(), P(), P(None, "col"))
    return jax.shard_map(
        on_device, mesh=mesh, in_specs=placed, out_specs=P(None, "row", "col"), check_vma=False
    )
```

```python
import numpy as np
import jax
import jax.numpy as jnp
from jax import lax
from jax.experimental import pallas as pl
from jax.experimental.pallas import tpu as pltpu
from jax.sharding import PartitionSpec as P

MESH = pl.DeviceIdType.MESH
ROWS, COLS = 32, 8
SEQS, LOCAL, D = 2, 2048, 1024
TILE = 256
TILES = LOCAL // TILE
STEP = 2
SEQ = ROWS * LOCAL
WIDTH = 64
CHANNELS = COLS * WIDTH
OUT = D // COLS
EPS = 1e-6
F32, BF16 = jnp.float32, jnp.bfloat16


def partner_channel(r, second):
    if r == 0:
        return 32 * second
    return WIDTH - r if second else r


def tables():
    n = np.arange(WIDTH)[:, None]
    analysis = np.zeros((2 * WIDTH, WIDTH))
    for r in range(ROWS):
        analysis[2 * r] = np.cos(2 * np.pi * n[:, 0] * r / WIDTH)
        analysis[2 * r + 1] = np.sin(2 * np.pi * n[:, 0] * r / WIDTH) if r else np.cos(np.pi * n[:, 0])
    a = np.arange(256)[:, None]
    p = np.arange(256)[None, :]
    turn = 2 * np.pi * (a * p % 256) / 256
    first = np.zeros((ROWS, 2, TILES, 4, 256))
    for e in range(2):
        first[:, e, :, 2 * e] = np.cos(turn).reshape(ROWS, TILES, 256)
        first[:, e, :, 2 * e + 1] = -np.sin(turn).reshape(ROWS, TILES, 256)
    first = first.reshape(2 * ROWS * TILES, 4, 2, 128).transpose(2, 0, 1, 3).reshape(2, 2 * ROWS * TILES, 512)
    twist = 2 * np.pi * (a * p) / SEQ
    twist = np.stack([np.cos(twist), -np.sin(twist)], axis=1).reshape(256, 2, 2, 128)
    twist = twist.transpose(2, 0, 1, 3).reshape(2, 256, 256)
    second = np.concatenate([np.cos(turn), np.sin(turn)], axis=1) / np.sqrt(SEQ * WIDTH)
    select = np.zeros((CHANNELS, CHANNELS))
    for r in range(ROWS):
        for ch in range(2):
            for c in range(COLS):
                select[r * 16 + ch * 8 + c, c * WIDTH + partner_channel(r, ch)] = 1.0
    return (
        jnp.asarray(analysis.T, BF16),
        jnp.asarray(first, BF16),
        jnp.asarray(twist, F32),
        jnp.asarray(second, BF16),
        jnp.asarray(select, BF16),
    )


def dot(x, y, dims=((1,), (0,))):
    return lax.dot_general(x, y, (dims, ((), ())), preferred_element_type=F32)


def kernel(
    tokens, gain, w_in, w_gate, w_spec, w_out, analysis, first, twist, second, select,
    out,
    tok, gain_v, w_in_v, wc, w_gate_v, w_spec_v, w_map, w_out_v,
    analysis_v, first_v, twist_v, second_v, select_v,
    turned, send1, recv1, mid, both, sendx, recvx, wide, send2, recv2, sig, result,
    tok_sem, load_sem, s1, r1, sx, rx, s2, r2, so, ro, own_o, swo, rwo, swn, rwn, swy, rwy, sf, rf,
):
    row, col = lax.axis_index("row"), lax.axis_index("col")
    chip, core = col // 2, col % 2

    def cols_of(c):
        return pl.ds(pl.multiple_of(c * OUT, OUT), OUT)

    loads = [
        pltpu.make_async_copy(src, dst, load_sem.at[i])
        for i, (src, dst) in enumerate(
            [
                (analysis, analysis_v), (w_in, w_in_v), (gain, gain_v),
                (first, first_v), (twist, twist_v), (second, second_v),
                (w_gate, w_gate_v), (w_out, w_out_v.at[:, cols_of(col)]),
                (w_spec, w_spec_v), (select, select_v),
            ]
        )
    ]

    def tile_copy(b, j):
        return pltpu.make_async_copy(
            tokens.at[b, pl.ds(pl.multiple_of(j * TILE, TILE), TILE)], tok.at[b, j], tok_sem.at[b, j]
        )

    for i in range(3):
        loads[i].start()

    peers_z = [((row // 4 + dz) % 8) * 4 for dz in range(8)]
    peers_y = [(row % 4 + dy) % 4 for dy in range(4)]
    peers_c = [(col + d) % COLS for d in range(COLS)]
    far_first = sorted(
        ((dz, dy) for dz in range(8) for dy in range(4) if dz or dy),
        key=lambda o: -(min(o[0], 8 - o[0]) + min(o[1], 4 - o[1])),
    )

    barrier = pltpu.get_barrier_semaphore()
    for dz, dy in far_first:
        pl.semaphore_signal(barrier, inc=1, device_id=(peers_z[dz] + peers_y[dy], col), device_id_type=MESH)
    for d in range(1, COLS):
        pl.semaphore_signal(barrier, inc=1, device_id=(row, peers_c[d]), device_id_type=MESH)

    for b in range(SEQS):
        for j in range(TILES):
            tile_copy(b, j).start()
    for i in range(3, 10):
        loads[i].start()

    for i in range(3):
        loads[i].wait()
    scaled = (w_in_v[...].astype(F32) * gain_v[...]).astype(BF16)
    wc[...] = dot(scaled, analysis_v[...], ((0,), (0,))).astype(BF16)

    def rows16(r):
        return pl.ds(pl.multiple_of(16 * r, 16), 16)

    def strided(ref, h, lo, hi, count, stride):
        rows = [ref[h, pl.ds(at, count, stride), :] for at in (lo, hi)]
        return jnp.concatenate(rows, axis=0).astype(BF16)

    def project(b):
        def tiles(i, _):
            for u in range(STEP):
                tile_copy(b, STEP * i + u).wait()
            for u in range(STEP):
                j = STEP * i + u
                t = tok[b, j]
                wide_t = t.astype(F32)
                inverse = lax.rsqrt(jnp.sum(wide_t * wide_t, axis=1, keepdims=True) * (1.0 / D) + EPS)
                flipped = jnp.transpose(dot(t, wc[...]) * inverse)[:WIDTH]
                for h in range(2):
                    turned[h, pl.ds(pl.multiple_of(j * WIDTH, WIDTH), WIDTH), :] = flipped[:, 128 * h : 128 * (h + 1)]
            return 0

        lax.fori_loop(0, TILES // STEP, tiles, 0)

        def pick(i, _):
            for u in range(8):
                r = 8 * i + u
                for h in range(2):
                    lanes = slice(128 * h, 128 * (h + 1))
                    send1[b, rows16(r), lanes] = strided(turned, h, 2 * r, 2 * r + 1, TILES, WIDTH)
            return 0

        lax.fori_loop(0, ROWS // 8, pick, 0)

    def row_send(src, dst, ssem, rsem):
        mine = rows16(row)
        for dz, dy in far_first:
            peer = peers_z[dz] + peers_y[dy]
            pltpu.make_async_remote_copy(
                src_ref=src.at[rows16(peer)], dst_ref=dst.at[mine],
                send_sem=ssem, recv_sem=rsem, device_id=(peer, col), device_id_type=MESH,
            ).start()
        dst[mine, :] = src[mine, :]

    def wait_bytes(ref, sem):
        pltpu.make_async_copy(ref, ref, sem).wait()

    most = pl.ds(0, 16 * (ROWS - 1))
    col_order = (4, 5, 3, 2, 6, 7, 1)

    def col_send(b, h):
        for d in col_order:
            peer = peers_c[d]
            pltpu.make_async_remote_copy(
                src_ref=sendx.at[b, h, peer], dst_ref=recvx.at[b, h, col],
                send_sem=sx.at[b, h], recv_sem=rx.at[b, h], device_id=(row, peer), device_id_type=MESH,
            ).start()
        recvx[b, h, col] = sendx[b, h, col]

    def fourier(b):
        lone = row == 0
        across = jnp.transpose(recv1[b])
        for h in range(2):
            y = dot(across, first_v[h])
            tr, ti = twist_v[h, :, :128], twist_v[h, :, 128:]
            ar, ai, br, bi = (y[:, 128 * i : 128 * (i + 1)] for i in range(4))
            pa, qa = ar * tr - ai * ti, ar * ti + ai * tr
            pb, qb = br * tr - bi * ti, br * ti + bi * tr
            both[h, :256, :128] = pa.astype(BF16)
            both[h, 256:, :128] = qa.astype(BF16)
            both[h, :256, 128:] = jnp.where(lone, pb, -qb).astype(BF16)
            both[h, 256:, 128:] = jnp.where(lone, qb, pb).astype(BF16)
            d = dot(second_v[...], both[h])
            da, db = d[:, :128], d[:, 128:]
            mid[h, :256] = jnp.where(lone, da, da - db)
            mid[h, 256:] = jnp.where(lone, db, da + db)
            for c in range(COLS):
                sendx[b, h, c] = strided(mid, h, c, 256 + c, ROWS, COLS)
            col_send(b, h)

    def regroup(b, h):
        for c in range(COLS):
            wide[h, c * WIDTH : (c + 1) * WIDTH, :] = recvx[b, h, c].astype(F32)

        def pick(i, _):
            for u in range(4):
                r = 4 * i + u
                send2[b, h, rows16(r), :] = strided(wide, h, r, ROWS + r, COLS, WIDTH)
            return 0

        lax.fori_loop(0, ROWS // 4, pick, 0)

    def gates(b):
        t = tok[b, col].astype(F32)
        inverse = lax.rsqrt(jnp.sum(t * t, axis=1, keepdims=True) * (1.0 / D) + EPS)
        normed = (t * inverse * gain_v[...]).astype(BF16)
        sig[b] = jax.nn.sigmoid(dot(normed, w_gate_v[...]))

    quarter = pl.ds(pl.multiple_of(row % 4 * 256, 256), 256)

    def shard_of(d):
        return cols_of((chip + d) % 4 * 2 + core)

    def share_out(rows, d, ssem, rsem, peer):
        return pltpu.make_async_remote_copy(
            src_ref=w_out_v.at[rows, shard_of(d)], dst_ref=w_out_v.at[rows, shard_of(d)],
            send_sem=ssem, recv_sem=rsem, device_id=peer, device_id_type=MESH,
        )

    def at_chip(d):
        return (row, (chip + d) % 4 * 2 + core)

    every = pl.ds(0, D)
    other_core = (row, chip * 2 + 1 - core)

    def finish(b, h):
        lanes = pl.ds(128 * h, 128)
        pre = dot(recv2[b, h], w_map[...], ((0,), (0,))).astype(BF16).astype(F32)
        mixed = (sig[b, lanes] * pre).astype(BF16)
        result[b, lanes] = dot(mixed, w_out_v[...]).astype(BF16)
        place = pl.ds(pl.multiple_of(col * TILE + 128 * h, 128), 128)

        for d in col_order:
            peer = peers_c[d]
            pltpu.make_async_remote_copy(
                src_ref=result.at[b, lanes, cols_of(peer)], dst_ref=out.at[b, place],
                send_sem=so.at[b, h], recv_sem=ro.at[b, h], device_id=(row, peer), device_id_type=MESH,
            ).start()
        pltpu.make_async_copy(result.at[b, lanes, cols_of(col)], out.at[b, place], own_o.at[b, h]).start()

    def forward(b):
        row_send(send1.at[b], recv1.at[b], s1.at[b], r1.at[b])

    def back(b, h):
        wait_bytes(recvx.at[b, h, pl.ds(0, COLS - 1)], rx.at[b, h])
        regroup(b, h)
        row_send(send2.at[b, h], recv2.at[b, h], s2.at[b, h], r2.at[b, h])

    project(0)
    pl.semaphore_wait(barrier, ROWS - 1 + COLS - 1)
    forward(0)
    loads[7].wait()
    share_out(quarter, 0, swo, rwo, at_chip(2)).start()
    share_out(every, 0, swn, rwn, at_chip(1)).start()
    share_out(every, 0, swn, rwn, at_chip(3)).start()
    share_out(every, 0, sf, rf, other_core).start()
    project(1)
    loads[6].wait()
    gates(0)
    loads[8].wait()
    loads[9].wait()
    w_map[...] = dot(select_v[...], w_spec_v[...]).astype(BF16)
    gates(1)
    forward(1)
    wait_bytes(w_out_v.at[pl.ds(0, 256), pl.ds(0, OUT)], rwo)
    for d in range(1, 4):
        share_out(quarter, 2, swy, rwy, (row // 4 * 4 + (row % 4 + d) % 4, col)).start()
    for i in range(3, 6):
        loads[i].wait()

    wait_bytes(recv1.at[0, most], r1.at[0])
    fourier(0)
    back(0, 0)
    back(0, 1)
    wait_bytes(recv1.at[1, most], r1.at[1])
    fourier(1)
    wait_bytes(w_out_v.at[:, pl.ds(0, 2 * OUT)], rwn)
    wait_bytes(w_out_v.at[pl.ds(0, 768), pl.ds(0, OUT)], rwy)
    for d in range(1, 4):
        share_out(every, d, sf, rf, other_core).start()
    back(1, 0)
    back(1, 1)
    wait_bytes(w_out_v.at[:, pl.ds(0, 4 * OUT)], rf)
    for b in range(SEQS):
        for h in range(2):
            wait_bytes(recv2.at[b, h, most], r2.at[b, h])
            finish(b, h)

    wait_bytes(w_out_v.at[pl.ds(0, 256), pl.ds(0, OUT)], swo)
    wait_bytes(w_out_v.at[:, pl.ds(0, 2 * OUT)], swn)
    wait_bytes(w_out_v.at[pl.ds(0, 768), pl.ds(0, OUT)], swy)
    wait_bytes(w_out_v.at[:, pl.ds(0, 4 * OUT)], sf)
    for b in range(SEQS):
        wait_bytes(send1.at[b, most], s1.at[b])
        for h in range(2):
            lanes = pl.ds(128 * h, 128)
            wait_bytes(sendx.at[b, h, pl.ds(0, COLS - 1)], sx.at[b, h])
            wait_bytes(send2.at[b, h, most], s2.at[b, h])
            wait_bytes(result.at[b, lanes, pl.ds(0, (COLS - 1) * OUT)], so.at[b, h])
            wait_bytes(out.at[b, pl.ds(0, (COLS - 1) * 128)], ro.at[b, h])
            wait_bytes(result.at[b, lanes, pl.ds(0, OUT)], own_o.at[b, h])


def on_device(tokens, norm_gain, w_fourier_in, w_gate, w_spectrum, w_output):
    dma = pltpu.SemaphoreType.DMA
    pair, halves = dma((SEQS,)), dma((SEQS, 2))
    scratch = [
        pltpu.VMEM((SEQS, TILES, TILE, D), BF16),
        pltpu.VMEM((1, D), F32),
        pltpu.VMEM((WIDTH, D), BF16),
        pltpu.VMEM((D, 2 * WIDTH), BF16),
        pltpu.VMEM((D, D), BF16),
        pltpu.VMEM((CHANNELS, D), BF16),
        pltpu.VMEM((CHANNELS, D), BF16),
        pltpu.VMEM((D, D), BF16),
        pltpu.VMEM((WIDTH, 2 * WIDTH), BF16),
        pltpu.VMEM((2, 512, 512), BF16),
        pltpu.VMEM((2, 256, 256), F32),
        pltpu.VMEM((256, 512), BF16),
        pltpu.VMEM((CHANNELS, CHANNELS), BF16),
        pltpu.VMEM((2, TILES * WIDTH, 128), F32),
        pltpu.VMEM((SEQS, 16 * ROWS, 256), BF16),
        pltpu.VMEM((SEQS, 16 * ROWS, 256), BF16),
        pltpu.VMEM((2, 512, 128), F32),
        pltpu.VMEM((2, 512, 256), BF16),
        pltpu.VMEM((SEQS, 2, COLS, WIDTH, 128), BF16),
        pltpu.VMEM((SEQS, 2, COLS, WIDTH, 128), BF16),
        pltpu.VMEM((2, COLS * WIDTH, 128), F32),
        pltpu.VMEM((SEQS, 2, 16 * ROWS, 128), BF16),
        pltpu.VMEM((SEQS, 2, 16 * ROWS, 128), BF16),
        pltpu.VMEM((SEQS, TILE, D), F32),
        pltpu.VMEM((SEQS, TILE, D), BF16),
        dma((SEQS, TILES)), dma((10,)),
        pair, pair, halves, halves, halves, halves, halves, halves, halves,
        dma, dma, dma, dma, dma, dma, dma, dma,
    ]
    anywhere = pl.BlockSpec(memory_space=pl.ANY)
    return pl.pallas_call(
        kernel,
        out_shape=pltpu.VMEM((SEQS, LOCAL, OUT), BF16),
        in_specs=[anywhere] * 11,
        out_specs=anywhere,
        scratch_shapes=scratch,
        compiler_params=pltpu.CompilerParams(
            collective_id=0, has_side_effects=True, vmem_limit_bytes=56 * 1024 * 1024
        ),
        name="fourier_mix",
    )(tokens, norm_gain.reshape(1, D), w_fourier_in.T, w_gate, w_spectrum, w_output, *tables())


def solution(mesh):
    placed = (P(None, "row", None), P(), P(None, "col"), P(), P(), P(None, "col"))
    return jax.shard_map(
        on_device, mesh=mesh, in_specs=placed, out_specs=P(None, "row", "col"), check_vma=False
    )
```

```python
import numpy as np
import jax
import jax.numpy as jnp
from jax import lax
from jax.experimental import pallas as pl
from jax.experimental.pallas import tpu as pltpu
from jax.sharding import PartitionSpec as P

MESH = pl.DeviceIdType.MESH
ROWS, COLS = 32, 8
SEQS, LOCAL, D = 2, 2048, 1024
TILE = 256
TILES = LOCAL // TILE
STEP = 2
SEQ = ROWS * LOCAL
WIDTH = 64
CHANNELS = COLS * WIDTH
OUT = D // COLS
EPS = 1e-6
F32, BF16 = jnp.float32, jnp.bfloat16


def partner_channel(r, second):
    if r == 0:
        return 32 * second
    return WIDTH - r if second else r


def tables():
    n = np.arange(WIDTH)[:, None]
    analysis = np.zeros((2 * WIDTH, WIDTH))
    for r in range(ROWS):
        analysis[2 * r] = np.cos(2 * np.pi * n[:, 0] * r / WIDTH)
        analysis[2 * r + 1] = np.sin(2 * np.pi * n[:, 0] * r / WIDTH) if r else np.cos(np.pi * n[:, 0])
    a = np.arange(256)[:, None]
    p = np.arange(256)[None, :]
    turn = 2 * np.pi * (a * p % 256) / 256
    first = np.zeros((ROWS, 2, TILES, 4, 256))
    for e in range(2):
        first[:, e, :, 2 * e] = np.cos(turn).reshape(ROWS, TILES, 256)
        first[:, e, :, 2 * e + 1] = -np.sin(turn).reshape(ROWS, TILES, 256)
    first = first.reshape(2 * ROWS * TILES, 4, 2, 128).transpose(2, 0, 1, 3).reshape(2, 2 * ROWS * TILES, 512)
    twist = 2 * np.pi * (a * p) / SEQ
    twist = np.stack([np.cos(twist), -np.sin(twist)], axis=1).reshape(256, 2, 2, 128)
    twist = twist.transpose(2, 0, 1, 3).reshape(2, 256, 256)
    second = np.concatenate([np.cos(turn), np.sin(turn)], axis=1) / np.sqrt(SEQ * WIDTH)
    select = np.zeros((CHANNELS, CHANNELS))
    for r in range(ROWS):
        for ch in range(2):
            for c in range(COLS):
                select[ch * 256 + r * 8 + c, c * WIDTH + partner_channel(r, ch)] = 1.0
    return (
        jnp.asarray(analysis.T, BF16),
        jnp.asarray(first, BF16),
        jnp.asarray(twist, F32),
        jnp.asarray(second, BF16),
        jnp.asarray(select, BF16),
    )


def dot(x, y, dims=((1,), (0,))):
    return lax.dot_general(x, y, (dims, ((), ())), preferred_element_type=F32)


def kernel(
    tokens, gain, w_in, w_gate, w_spec, w_out, analysis, first, twist, second, select,
    out,
    tok, gain_v, w_in_v, wc, w_gate_v, w_spec_v, w_map, w_out_v,
    analysis_v, first_v, twist_v, second_v, select_v,
    turned, send1, recv1, mid, both, sendx, recvx, wide, send2, recv2, sig, result,
    tok_sem, load_sem, s1, r1, sx, rx, s2, r2, so, ro, own_o, swo, rwo, swn, rwn, swy, rwy, sf, rf,
):
    row, col = lax.axis_index("row"), lax.axis_index("col")
    chip, core = col // 2, col % 2

    def cols_of(c):
        return pl.ds(pl.multiple_of(c * OUT, OUT), OUT)

    loads = [
        pltpu.make_async_copy(src, dst, load_sem.at[i])
        for i, (src, dst) in enumerate(
            [
                (analysis, analysis_v), (w_in, w_in_v), (gain, gain_v),
                (first, first_v), (twist, twist_v), (second, second_v),
                (w_gate, w_gate_v), (w_out, w_out_v.at[:, cols_of(col)]),
                (w_spec, w_spec_v), (select, select_v),
            ]
        )
    ]

    def tile_copy(b, j):
        return pltpu.make_async_copy(
            tokens.at[b, pl.ds(pl.multiple_of(j * TILE, TILE), TILE)], tok.at[b, j], tok_sem.at[b, j]
        )

    for i in range(3):
        loads[i].start()

    peers_z = [((row // 4 + dz) % 8) * 4 for dz in range(8)]
    peers_y = [(row % 4 + dy) % 4 for dy in range(4)]
    peers_c = [(col + d) % COLS for d in range(COLS)]
    far_first = sorted(
        ((dz, dy) for dz in range(8) for dy in range(4) if dz or dy),
        key=lambda o: -(min(o[0], 8 - o[0]) + min(o[1], 4 - o[1])),
    )
    paired = []
    for dz, dy in far_first:
        for one in ((dz, dy), (-dz % 8, -dy % 4)):
            if one not in paired:
                paired.append(one)

    barrier = pltpu.get_barrier_semaphore()
    for dz, dy in far_first:
        pl.semaphore_signal(barrier, inc=1, device_id=(peers_z[dz] + peers_y[dy], col), device_id_type=MESH)
    for d in range(1, COLS):
        pl.semaphore_signal(barrier, inc=1, device_id=(row, peers_c[d]), device_id_type=MESH)

    for b in range(SEQS):
        for j in range(TILES):
            tile_copy(b, j).start()
    for i in range(3, 10):
        loads[i].start()

    for i in range(3):
        loads[i].wait()
    scaled = (w_in_v[...].astype(F32) * gain_v[...]).astype(BF16)
    wc[...] = dot(scaled, analysis_v[...], ((0,), (0,))).astype(BF16)

    def rows16(r):
        return pl.ds(pl.multiple_of(16 * r, 16), 16)

    def strided(ref, h, lo, hi, count, stride):
        rows = [ref[h, pl.ds(at, count, stride), :] for at in (lo, hi)]
        return jnp.concatenate(rows, axis=0).astype(BF16)

    def project(b):
        def tiles(i, _):
            for u in range(STEP):
                tile_copy(b, STEP * i + u).wait()
            for u in range(STEP):
                j = STEP * i + u
                t = tok[b, j]
                wide_t = t.astype(F32)
                inverse = lax.rsqrt(jnp.sum(wide_t * wide_t, axis=1, keepdims=True) * (1.0 / D) + EPS)
                flipped = jnp.transpose(dot(t, wc[...]) * inverse)[:WIDTH]
                for h in range(2):
                    turned[h, pl.ds(pl.multiple_of(j * WIDTH, WIDTH), WIDTH), :] = flipped[:, 128 * h : 128 * (h + 1)]
            return 0

        lax.fori_loop(0, TILES // STEP, tiles, 0)

        def pick(i, _):
            for u in range(8):
                r = 8 * i + u
                for h in range(2):
                    lanes = slice(128 * h, 128 * (h + 1))
                    send1[b, rows16(r), lanes] = strided(turned, h, 2 * r, 2 * r + 1, TILES, WIDTH)
            return 0

        lax.fori_loop(0, ROWS // 8, pick, 0)

    def row_send(src, dst, ssem, rsem, block):
        mine = block(row)
        for dz, dy in paired:
            peer = peers_z[dz] + peers_y[dy]
            pltpu.make_async_remote_copy(
                src_ref=src.at[block(peer)], dst_ref=dst.at[mine],
                send_sem=ssem, recv_sem=rsem, device_id=(peer, col), device_id_type=MESH,
            ).start()
        dst[mine] = src[mine]

    def wait_bytes(ref, sem):
        pltpu.make_async_copy(ref, ref, sem).wait()

    most = pl.ds(0, 16 * (ROWS - 1))
    col_order = (4, 5, 3, 2, 6, 7, 1)

    def col_send(b, h):
        for d in col_order:
            peer = peers_c[d]
            pltpu.make_async_remote_copy(
                src_ref=sendx.at[b, h, peer], dst_ref=recvx.at[b, h, col],
                send_sem=sx.at[b, h], recv_sem=rx.at[b, h], device_id=(row, peer), device_id_type=MESH,
            ).start()
        recvx[b, h, col] = sendx[b, h, col]

    def fourier(b):
        lone = row == 0
        across = jnp.transpose(recv1[b])
        for h in range(2):
            y = dot(across, first_v[h])
            tr, ti = twist_v[h, :, :128], twist_v[h, :, 128:]
            ar, ai, br, bi = (y[:, 128 * i : 128 * (i + 1)] for i in range(4))
            pa, qa = ar * tr - ai * ti, ar * ti + ai * tr
            pb, qb = br * tr - bi * ti, br * ti + bi * tr
            both[h, :256, :128] = pa.astype(BF16)
            both[h, 256:, :128] = qa.astype(BF16)
            both[h, :256, 128:] = jnp.where(lone, pb, -qb).astype(BF16)
            both[h, 256:, 128:] = jnp.where(lone, qb, pb).astype(BF16)
            d = dot(second_v[...], both[h])
            da, db = d[:, :128], d[:, 128:]
            mid[h, :256] = jnp.where(lone, da, da - db)
            mid[h, 256:] = jnp.where(lone, db, da + db)
            for c in range(COLS):
                sendx[b, h, c] = strided(mid, h, c, 256 + c, ROWS, COLS)
            col_send(b, h)

    def regroup(b, h):
        for c in range(COLS):
            wide[h, c * WIDTH : (c + 1) * WIDTH, :] = recvx[b, h, c].astype(F32)

        left = lax.broadcasted_iota(jnp.int32, (COLS, 128), 1) < 64

        def pick(i, _):
            for u in range(16):
                r = 16 * i + u
                lo, hi = wide[h, pl.ds(r, COLS, WIDTH), :], wide[h, pl.ds(ROWS + r, COLS, WIDTH), :]
                send2[b, 2 * h, r] = jnp.where(left, lo, pltpu.roll(hi, 64, 1)).astype(BF16)
                send2[b, 2 * h + 1, r] = jnp.where(left, pltpu.roll(lo, 64, 1), hi).astype(BF16)
            return 0

        lax.fori_loop(0, ROWS // 16, pick, 0)

    def gates(b):
        t = tok[b, col].astype(F32)
        inverse = lax.rsqrt(jnp.sum(t * t, axis=1, keepdims=True) * (1.0 / D) + EPS)
        normed = (t * inverse * gain_v[...]).astype(BF16)
        sig[b] = jax.nn.sigmoid(dot(normed, w_gate_v[...]))

    quarter = pl.ds(pl.multiple_of(row % 4 * 256, 256), 256)

    def shard_of(d):
        return cols_of((chip + d) % 4 * 2 + core)

    def share_out(rows, d, ssem, rsem, peer):
        return pltpu.make_async_remote_copy(
            src_ref=w_out_v.at[rows, shard_of(d)], dst_ref=w_out_v.at[rows, shard_of(d)],
            send_sem=ssem, recv_sem=rsem, device_id=peer, device_id_type=MESH,
        )

    def at_chip(d):
        return (row, (chip + d) % 4 * 2 + core)

    every = pl.ds(0, D)
    other_core = (row, chip * 2 + 1 - core)

    def finish(b, t):
        wait_bytes(recv2.at[b, t, pl.ds(0, ROWS - 1)], r2.at[b, t])
        part = pl.ds(64 * t, 64)
        block = jnp.transpose(recv2[b, t].astype(F32).reshape(COLS * ROWS, 128)).astype(BF16)
        pre = dot(block[:64], w_map[:256]) + dot(block[64:], w_map[256:])
        mixed = (sig[b, part] * pre.astype(BF16).astype(F32)).astype(BF16)
        result[b, part] = dot(mixed, w_out_v[...]).astype(BF16)
        place = pl.ds(pl.multiple_of(col * TILE + 64 * t, 64), 64)

        for d in col_order:
            peer = peers_c[d]
            pltpu.make_async_remote_copy(
                src_ref=result.at[b, part, cols_of(peer)], dst_ref=out.at[b, place],
                send_sem=so.at[b, t], recv_sem=ro.at[b, t], device_id=(row, peer), device_id_type=MESH,
            ).start()
        pltpu.make_async_copy(result.at[b, part, cols_of(col)], out.at[b, place], own_o.at[b, t]).start()

    def forward(b):
        row_send(send1.at[b], recv1.at[b], s1.at[b], r1.at[b], rows16)

    def back(b, h):
        wait_bytes(recvx.at[b, h, pl.ds(0, COLS - 1)], rx.at[b, h])
        regroup(b, h)
        for t in (2 * h, 2 * h + 1):
            row_send(send2.at[b, t], recv2.at[b, t], s2.at[b, t], r2.at[b, t], lambda r: r)

    project(0)
    pl.semaphore_wait(barrier, ROWS - 1 + COLS - 1)
    forward(0)
    loads[7].wait()
    share_out(quarter, 0, swo, rwo, at_chip(2)).start()
    share_out(every, 0, swn, rwn, at_chip(1)).start()
    share_out(every, 0, swn, rwn, at_chip(3)).start()
    share_out(every, 0, sf, rf, other_core).start()
    project(1)
    loads[6].wait()
    gates(0)
    loads[8].wait()
    loads[9].wait()
    w_map[...] = dot(select_v[...], w_spec_v[...]).astype(BF16)
    gates(1)
    forward(1)
    wait_bytes(w_out_v.at[pl.ds(0, 256), pl.ds(0, OUT)], rwo)
    for d in range(1, 4):
        share_out(quarter, 2, swy, rwy, (row // 4 * 4 + (row % 4 + d) % 4, col)).start()
    for i in range(3, 6):
        loads[i].wait()

    wait_bytes(recv1.at[0, most], r1.at[0])
    fourier(0)
    back(0, 0)
    wait_bytes(recv1.at[1, most], r1.at[1])
    fourier(1)
    back(0, 1)
    wait_bytes(w_out_v.at[:, pl.ds(0, 2 * OUT)], rwn)
    wait_bytes(w_out_v.at[pl.ds(0, 768), pl.ds(0, OUT)], rwy)
    for d in range(1, 4):
        share_out(every, d, sf, rf, other_core).start()
    wait_bytes(w_out_v.at[:, pl.ds(0, 4 * OUT)], rf)
    back(1, 0)
    finish(0, 0)
    back(1, 1)
    for b, t in ((0, 1), (0, 2), (0, 3), (1, 0), (1, 1), (1, 2), (1, 3)):
        finish(b, t)

    wait_bytes(w_out_v.at[pl.ds(0, 256), pl.ds(0, OUT)], swo)
    wait_bytes(w_out_v.at[:, pl.ds(0, 2 * OUT)], swn)
    wait_bytes(w_out_v.at[pl.ds(0, 768), pl.ds(0, OUT)], swy)
    wait_bytes(w_out_v.at[:, pl.ds(0, 4 * OUT)], sf)
    for b in range(SEQS):
        wait_bytes(send1.at[b, most], s1.at[b])
        for h in range(2):
            wait_bytes(sendx.at[b, h, pl.ds(0, COLS - 1)], sx.at[b, h])
        for t in range(4):
            part = pl.ds(64 * t, 64)
            wait_bytes(send2.at[b, t, pl.ds(0, ROWS - 1)], s2.at[b, t])
            wait_bytes(result.at[b, part, pl.ds(0, (COLS - 1) * OUT)], so.at[b, t])
            wait_bytes(out.at[b, pl.ds(0, (COLS - 1) * 64)], ro.at[b, t])
            wait_bytes(result.at[b, part, pl.ds(0, OUT)], own_o.at[b, t])


def on_device(tokens, norm_gain, w_fourier_in, w_gate, w_spectrum, w_output):
    dma = pltpu.SemaphoreType.DMA
    pair, halves, quarters = dma((SEQS,)), dma((SEQS, 2)), dma((SEQS, 4))
    scratch = [
        pltpu.VMEM((SEQS, TILES, TILE, D), BF16),
        pltpu.VMEM((1, D), F32),
        pltpu.VMEM((WIDTH, D), BF16),
        pltpu.VMEM((D, 2 * WIDTH), BF16),
        pltpu.VMEM((D, D), BF16),
        pltpu.VMEM((CHANNELS, D), BF16),
        pltpu.VMEM((CHANNELS, D), BF16),
        pltpu.VMEM((D, D), BF16),
        pltpu.VMEM((WIDTH, 2 * WIDTH), BF16),
        pltpu.VMEM((2, 512, 512), BF16),
        pltpu.VMEM((2, 256, 256), F32),
        pltpu.VMEM((256, 512), BF16),
        pltpu.VMEM((CHANNELS, CHANNELS), BF16),
        pltpu.VMEM((2, TILES * WIDTH, 128), F32),
        pltpu.VMEM((SEQS, 16 * ROWS, 256), BF16),
        pltpu.VMEM((SEQS, 16 * ROWS, 256), BF16),
        pltpu.VMEM((2, 512, 128), F32),
        pltpu.VMEM((2, 512, 256), BF16),
        pltpu.VMEM((SEQS, 2, COLS, WIDTH, 128), BF16),
        pltpu.VMEM((SEQS, 2, COLS, WIDTH, 128), BF16),
        pltpu.VMEM((2, COLS * WIDTH, 128), F32),
        pltpu.VMEM((SEQS, 4, ROWS, 8, 128), BF16),
        pltpu.VMEM((SEQS, 4, ROWS, 8, 128), BF16),
        pltpu.VMEM((SEQS, TILE, D), F32),
        pltpu.VMEM((SEQS, TILE, D), BF16),
        dma((SEQS, TILES)), dma((10,)),
        pair, pair, halves, halves, quarters, quarters, quarters, quarters, quarters,
        dma, dma, dma, dma, dma, dma, dma, dma,
    ]
    anywhere = pl.BlockSpec(memory_space=pl.ANY)
    return pl.pallas_call(
        kernel,
        out_shape=pltpu.VMEM((SEQS, LOCAL, OUT), BF16),
        in_specs=[anywhere] * 11,
        out_specs=anywhere,
        scratch_shapes=scratch,
        compiler_params=pltpu.CompilerParams(
            collective_id=0, has_side_effects=True, vmem_limit_bytes=56 * 1024 * 1024
        ),
        name="fourier_mix",
    )(tokens, norm_gain.reshape(1, D), w_fourier_in.T, w_gate, w_spectrum, w_output, *tables())


def solution(mesh):
    placed = (P(None, "row", None), P(), P(None, "col"), P(), P(), P(None, "col"))
    return jax.shard_map(
        on_device, mesh=mesh, in_specs=placed, out_specs=P(None, "row", "col"), check_vma=False
    )
```

```python
import numpy as np
import jax
import jax.numpy as jnp
from jax import lax
from jax.experimental import pallas as pl
from jax.experimental.pallas import tpu as pltpu
from jax.sharding import PartitionSpec as P

MESH = pl.DeviceIdType.MESH
ROWS, COLS = 32, 8
SEQS, LOCAL, D = 2, 2048, 1024
TILE = 256
TILES = LOCAL // TILE
STEP = 2
SEQ = ROWS * LOCAL
WIDTH = 64
CHANNELS = COLS * WIDTH
OUT = D // COLS
EPS = 1e-6
F32, BF16 = jnp.float32, jnp.bfloat16


def partner_channel(r, second):
    if r == 0:
        return 32 * second
    return WIDTH - r if second else r


def tables():
    n = np.arange(WIDTH)[:, None]
    analysis = np.zeros((2 * WIDTH, WIDTH))
    for r in range(ROWS):
        analysis[2 * r] = np.cos(2 * np.pi * n[:, 0] * r / WIDTH)
        analysis[2 * r + 1] = np.sin(2 * np.pi * n[:, 0] * r / WIDTH) if r else np.cos(np.pi * n[:, 0])
    a = np.arange(256)[:, None]
    p = np.arange(256)[None, :]
    turn = 2 * np.pi * (a * p % 256) / 256
    first = np.zeros((ROWS, 2, TILES, 4, 256))
    for e in range(2):
        first[:, e, :, 2 * e] = np.cos(turn).reshape(ROWS, TILES, 256)
        first[:, e, :, 2 * e + 1] = -np.sin(turn).reshape(ROWS, TILES, 256)
    first = first.reshape(2 * ROWS * TILES, 4, 2, 128).transpose(2, 0, 1, 3).reshape(2, 2 * ROWS * TILES, 512)
    twist = 2 * np.pi * (a * p) / SEQ
    twist = np.stack([np.cos(twist), -np.sin(twist)], axis=1).reshape(256, 2, 2, 128)
    twist = twist.transpose(2, 0, 1, 3).reshape(2, 256, 256)
    second = np.concatenate([np.cos(turn), np.sin(turn)], axis=1) / np.sqrt(SEQ * WIDTH)
    select = np.zeros((CHANNELS, CHANNELS))
    for r in range(ROWS):
        for ch in range(2):
            for c in range(COLS):
                select[ch * 256 + r * 8 + c, c * WIDTH + partner_channel(r, ch)] = 1.0
    return (
        jnp.asarray(analysis.T, BF16),
        jnp.asarray(first, BF16),
        jnp.asarray(twist, F32),
        jnp.asarray(second, BF16),
        jnp.asarray(select, BF16),
    )


def dot(x, y, dims=((1,), (0,))):
    return lax.dot_general(x, y, (dims, ((), ())), preferred_element_type=F32)


def kernel(
    tokens, gain, w_in, w_gate, w_spec, w_out, analysis, first, twist, second, select,
    out,
    tok, gain_v, w_in_v, wc, w_gate_v, w_spec_v, w_map, w_out_v,
    analysis_v, first_v, twist_v, second_v, select_v,
    turned, send1, recv1, mid, both, sendx, recvx, wide, send2, recv2, sig, result,
    tok_sem, load_sem, s1, r1, sx, rx, s2, r2, so, ro, own_o, swo, rwo, swn, rwn, swy, rwy, sf, rf,
):
    row, col = lax.axis_index("row"), lax.axis_index("col")
    chip, core = col // 2, col % 2

    def cols_of(c):
        return pl.ds(pl.multiple_of(c * OUT, OUT), OUT)

    loads = [
        pltpu.make_async_copy(src, dst, load_sem.at[i])
        for i, (src, dst) in enumerate(
            [
                (analysis, analysis_v), (w_in, w_in_v), (gain, gain_v),
                (first, first_v), (twist, twist_v), (second, second_v),
                (w_gate, w_gate_v), (w_out, w_out_v.at[:, cols_of(col)]),
                (w_spec, w_spec_v), (select, select_v),
            ]
        )
    ]

    def tile_copy(b, j):
        return pltpu.make_async_copy(
            tokens.at[b, pl.ds(pl.multiple_of(j * TILE, TILE), TILE)], tok.at[b, j], tok_sem.at[b, j]
        )

    for i in range(3):
        loads[i].start()

    peers_z = [((row // 4 + dz) % 8) * 4 for dz in range(8)]
    peers_y = [(row % 4 + dy) % 4 for dy in range(4)]
    peers_c = [(col + d) % COLS for d in range(COLS)]
    far_first = sorted(
        ((dz, dy) for dz in range(8) for dy in range(4) if dz or dy),
        key=lambda o: -(min(o[0], 8 - o[0]) + min(o[1], 4 - o[1])),
    )
    paired = []
    for dz, dy in far_first:
        for one in ((dz, dy), (-dz % 8, -dy % 4)):
            if one not in paired:
                paired.append(one)

    barrier = pltpu.get_barrier_semaphore()
    for dz, dy in far_first:
        pl.semaphore_signal(barrier, inc=1, device_id=(peers_z[dz] + peers_y[dy], col), device_id_type=MESH)
    for d in range(1, COLS):
        pl.semaphore_signal(barrier, inc=1, device_id=(row, peers_c[d]), device_id_type=MESH)

    for b in range(SEQS):
        for j in range(TILES):
            tile_copy(b, j).start()
    for i in range(3, 10):
        loads[i].start()

    for i in range(3):
        loads[i].wait()
    scaled = (w_in_v[...].astype(F32) * gain_v[...]).astype(BF16)
    wc[...] = dot(scaled, analysis_v[...], ((0,), (0,))).astype(BF16)

    def rows16(r):
        return pl.ds(pl.multiple_of(16 * r, 16), 16)

    def strided(ref, h, lo, hi, count, stride):
        rows = [ref[h, pl.ds(at, count, stride), :] for at in (lo, hi)]
        return jnp.concatenate(rows, axis=0).astype(BF16)

    def project(b):
        def tiles(i, _):
            for u in range(STEP):
                tile_copy(b, STEP * i + u).wait()
            for u in range(STEP):
                j = STEP * i + u
                t = tok[b, j]
                wide_t = t.astype(F32)
                inverse = lax.rsqrt(jnp.sum(wide_t * wide_t, axis=1, keepdims=True) * (1.0 / D) + EPS)
                flipped = jnp.transpose(dot(t, wc[...]) * inverse)[:WIDTH]
                for h in range(2):
                    turned[h, pl.ds(pl.multiple_of(j * WIDTH, WIDTH), WIDTH), :] = flipped[:, 128 * h : 128 * (h + 1)]
            return 0

        lax.fori_loop(0, TILES // STEP, tiles, 0)

        def pick(i, _):
            for u in range(8):
                r = 8 * i + u
                for h in range(2):
                    lanes = slice(128 * h, 128 * (h + 1))
                    send1[b, rows16(r), lanes] = strided(turned, h, 2 * r, 2 * r + 1, TILES, WIDTH)
            return 0

        lax.fori_loop(0, ROWS // 8, pick, 0)

    def row_send(src, dst, ssem, rsem, block):
        mine = block(row)
        for dz, dy in paired:
            peer = peers_z[dz] + peers_y[dy]
            pltpu.make_async_remote_copy(
                src_ref=src.at[block(peer)], dst_ref=dst.at[mine],
                send_sem=ssem, recv_sem=rsem, device_id=(peer, col), device_id_type=MESH,
            ).start()
        dst[mine] = src[mine]

    def wait_bytes(ref, sem):
        pltpu.make_async_copy(ref, ref, sem).wait()

    most = pl.ds(0, 16 * (ROWS - 1))
    col_order = (4, 5, 3, 2, 6, 7, 1)

    def col_send(b, h):
        for d in col_order:
            peer = peers_c[d]
            pltpu.make_async_remote_copy(
                src_ref=sendx.at[b, h, peer], dst_ref=recvx.at[b, h, col],
                send_sem=sx.at[b, h], recv_sem=rx.at[b, h], device_id=(row, peer), device_id_type=MESH,
            ).start()
        recvx[b, h, col] = sendx[b, h, col]

    def fourier(b):
        lone = row == 0
        across = jnp.transpose(recv1[b])
        for h in range(2):
            y = dot(across, first_v[h])
            tr, ti = twist_v[h, :, :128], twist_v[h, :, 128:]
            ar, ai, br, bi = (y[:, 128 * i : 128 * (i + 1)] for i in range(4))
            pa, qa = ar * tr - ai * ti, ar * ti + ai * tr
            pb, qb = br * tr - bi * ti, br * ti + bi * tr
            both[h, :256, :128] = pa.astype(BF16)
            both[h, 256:, :128] = qa.astype(BF16)
            both[h, :256, 128:] = jnp.where(lone, pb, -qb).astype(BF16)
            both[h, 256:, 128:] = jnp.where(lone, qb, pb).astype(BF16)
            d = dot(second_v[...], both[h])
            da, db = d[:, :128], d[:, 128:]
            mid[h, :256] = jnp.where(lone, da, da - db)
            mid[h, 256:] = jnp.where(lone, db, da + db)
            for c in range(COLS):
                sendx[b, h, c] = strided(mid, h, c, 256 + c, ROWS, COLS)
            col_send(b, h)

    def regroup(b, h):
        for c in range(COLS):
            wide[h, c * WIDTH : (c + 1) * WIDTH, :] = recvx[b, h, c].astype(F32)

        left = lax.broadcasted_iota(jnp.int32, (COLS, 128), 1) < 64

        def pick(i, _):
            for u in range(16):
                r = 16 * i + u
                lo, hi = wide[h, pl.ds(r, COLS, WIDTH), :], wide[h, pl.ds(ROWS + r, COLS, WIDTH), :]
                send2[b, 2 * h, r] = jnp.where(left, lo, pltpu.roll(hi, 64, 1)).astype(BF16)
                send2[b, 2 * h + 1, r] = jnp.where(left, pltpu.roll(lo, 64, 1), hi).astype(BF16)
            return 0

        lax.fori_loop(0, ROWS // 16, pick, 0)

    def gates(b):
        t = tok[b, col].astype(F32)
        inverse = lax.rsqrt(jnp.sum(t * t, axis=1, keepdims=True) * (1.0 / D) + EPS)
        normed = (t * inverse * gain_v[...]).astype(BF16)
        sig[b] = jax.nn.sigmoid(dot(normed, w_gate_v[...]))

    quarter = pl.ds(pl.multiple_of(row % 4 * 256, 256), 256)

    def shard_of(d):
        return cols_of((chip + d) % 4 * 2 + core)

    def share_out(rows, d, ssem, rsem, peer):
        return pltpu.make_async_remote_copy(
            src_ref=w_out_v.at[rows, shard_of(d)], dst_ref=w_out_v.at[rows, shard_of(d)],
            send_sem=ssem, recv_sem=rsem, device_id=peer, device_id_type=MESH,
        )

    def at_chip(d):
        return (row, (chip + d) % 4 * 2 + core)

    every = pl.ds(0, D)
    other_core = (row, chip * 2 + 1 - core)

    def finish(b, t):
        wait_bytes(recv2.at[b, t, pl.ds(0, ROWS - 1)], r2.at[b, t])
        part = pl.ds(64 * t, 64)
        block = jnp.transpose(recv2[b, t].reshape(COLS * ROWS, 128))
        pre = dot(block[:64], w_map[:256]) + dot(block[64:], w_map[256:])
        mixed = (sig[b, part] * pre.astype(BF16).astype(F32)).astype(BF16)
        result[b, part] = dot(mixed, w_out_v[...]).astype(BF16)
        place = pl.ds(pl.multiple_of(col * TILE + 64 * t, 64), 64)

        for d in col_order:
            peer = peers_c[d]
            pltpu.make_async_remote_copy(
                src_ref=result.at[b, part, cols_of(peer)], dst_ref=out.at[b, place],
                send_sem=so.at[b, t], recv_sem=ro.at[b, t], device_id=(row, peer), device_id_type=MESH,
            ).start()
        pltpu.make_async_copy(result.at[b, part, cols_of(col)], out.at[b, place], own_o.at[b, t]).start()

    def forward(b):
        row_send(send1.at[b], recv1.at[b], s1.at[b], r1.at[b], rows16)

    def back(b, h):
        wait_bytes(recvx.at[b, h, pl.ds(0, COLS - 1)], rx.at[b, h])
        regroup(b, h)
        for t in (2 * h, 2 * h + 1):
            row_send(send2.at[b, t], recv2.at[b, t], s2.at[b, t], r2.at[b, t], lambda r: r)

    project(0)
    pl.semaphore_wait(barrier, ROWS - 1 + COLS - 1)
    forward(0)
    loads[7].wait()
    share_out(quarter, 0, swo, rwo, at_chip(2)).start()
    share_out(every, 0, swn, rwn, at_chip(1)).start()
    share_out(every, 0, swn, rwn, at_chip(3)).start()
    share_out(every, 0, sf, rf, other_core).start()
    project(1)
    loads[6].wait()
    gates(0)
    loads[8].wait()
    loads[9].wait()
    w_map[...] = dot(select_v[...], w_spec_v[...]).astype(BF16)
    gates(1)
    forward(1)
    wait_bytes(w_out_v.at[pl.ds(0, 256), pl.ds(0, OUT)], rwo)
    for d in range(1, 4):
        share_out(quarter, 2, swy, rwy, (row // 4 * 4 + (row % 4 + d) % 4, col)).start()
    for i in range(3, 6):
        loads[i].wait()

    wait_bytes(recv1.at[0, most], r1.at[0])
    fourier(0)
    back(0, 0)
    wait_bytes(recv1.at[1, most], r1.at[1])
    fourier(1)
    back(0, 1)
    wait_bytes(w_out_v.at[:, pl.ds(0, 2 * OUT)], rwn)
    wait_bytes(w_out_v.at[pl.ds(0, 768), pl.ds(0, OUT)], rwy)
    for d in range(1, 4):
        share_out(every, d, sf, rf, other_core).start()
    wait_bytes(w_out_v.at[:, pl.ds(0, 4 * OUT)], rf)
    back(1, 0)
    finish(0, 0)
    back(1, 1)
    for b, t in ((0, 1), (0, 2), (0, 3), (1, 0), (1, 1), (1, 2), (1, 3)):
        finish(b, t)

    wait_bytes(w_out_v.at[pl.ds(0, 256), pl.ds(0, OUT)], swo)
    wait_bytes(w_out_v.at[:, pl.ds(0, 2 * OUT)], swn)
    wait_bytes(w_out_v.at[pl.ds(0, 768), pl.ds(0, OUT)], swy)
    wait_bytes(w_out_v.at[:, pl.ds(0, 4 * OUT)], sf)
    for b in range(SEQS):
        wait_bytes(send1.at[b, most], s1.at[b])
        for h in range(2):
            wait_bytes(sendx.at[b, h, pl.ds(0, COLS - 1)], sx.at[b, h])
        for t in range(4):
            part = pl.ds(64 * t, 64)
            wait_bytes(send2.at[b, t, pl.ds(0, ROWS - 1)], s2.at[b, t])
            wait_bytes(result.at[b, part, pl.ds(0, (COLS - 1) * OUT)], so.at[b, t])
            wait_bytes(out.at[b, pl.ds(0, (COLS - 1) * 64)], ro.at[b, t])
            wait_bytes(result.at[b, part, pl.ds(0, OUT)], own_o.at[b, t])


def on_device(tokens, norm_gain, w_fourier_in, w_gate, w_spectrum, w_output):
    dma = pltpu.SemaphoreType.DMA
    pair, halves, quarters = dma((SEQS,)), dma((SEQS, 2)), dma((SEQS, 4))
    scratch = [
        pltpu.VMEM((SEQS, TILES, TILE, D), BF16),
        pltpu.VMEM((1, D), F32),
        pltpu.VMEM((WIDTH, D), BF16),
        pltpu.VMEM((D, 2 * WIDTH), BF16),
        pltpu.VMEM((D, D), BF16),
        pltpu.VMEM((CHANNELS, D), BF16),
        pltpu.VMEM((CHANNELS, D), BF16),
        pltpu.VMEM((D, D), BF16),
        pltpu.VMEM((WIDTH, 2 * WIDTH), BF16),
        pltpu.VMEM((2, 512, 512), BF16),
        pltpu.VMEM((2, 256, 256), F32),
        pltpu.VMEM((256, 512), BF16),
        pltpu.VMEM((CHANNELS, CHANNELS), BF16),
        pltpu.VMEM((2, TILES * WIDTH, 128), F32),
        pltpu.VMEM((SEQS, 16 * ROWS, 256), BF16),
        pltpu.VMEM((SEQS, 16 * ROWS, 256), BF16),
        pltpu.VMEM((2, 512, 128), F32),
        pltpu.VMEM((2, 512, 256), BF16),
        pltpu.VMEM((SEQS, 2, COLS, WIDTH, 128), BF16),
        pltpu.VMEM((SEQS, 2, COLS, WIDTH, 128), BF16),
        pltpu.VMEM((2, COLS * WIDTH, 128), F32),
        pltpu.VMEM((SEQS, 4, ROWS, 8, 128), BF16),
        pltpu.VMEM((SEQS, 4, ROWS, 8, 128), BF16),
        pltpu.VMEM((SEQS, TILE, D), F32),
        pltpu.VMEM((SEQS, TILE, D), BF16),
        dma((SEQS, TILES)), dma((10,)),
        pair, pair, halves, halves, quarters, quarters, quarters, quarters, quarters,
        dma, dma, dma, dma, dma, dma, dma, dma,
    ]
    anywhere = pl.BlockSpec(memory_space=pl.ANY)
    return pl.pallas_call(
        kernel,
        out_shape=pltpu.VMEM((SEQS, LOCAL, OUT), BF16),
        in_specs=[anywhere] * 11,
        out_specs=anywhere,
        scratch_shapes=scratch,
        compiler_params=pltpu.CompilerParams(
            collective_id=0, has_side_effects=True, vmem_limit_bytes=56 * 1024 * 1024
        ),
        name="fourier_mix",
    )(tokens, norm_gain.reshape(1, D), w_fourier_in.T, w_gate, w_spectrum, w_output, *tables())


def solution(mesh):
    placed = (P(None, "row", None), P(), P(None, "col"), P(), P(), P(None, "col"))
    return jax.shard_map(
        on_device, mesh=mesh, in_specs=placed, out_specs=P(None, "row", "col"), check_vma=False
    )
```

```python
import numpy as np
import jax
import jax.numpy as jnp
from jax import lax
from jax.experimental import pallas as pl
from jax.experimental.pallas import tpu as pltpu
from jax.sharding import PartitionSpec as P

MESH = pl.DeviceIdType.MESH
ROWS, COLS = 32, 8
SEQS, LOCAL, D = 2, 2048, 1024
TILE = 256
TILES = LOCAL // TILE
STEP = 2
SEQ = ROWS * LOCAL
WIDTH = 64
CHANNELS = COLS * WIDTH
OUT = D // COLS
EPS = 1e-6
F32, BF16 = jnp.float32, jnp.bfloat16


def partner_channel(r, second):
    if r == 0:
        return 32 * second
    return WIDTH - r if second else r


def tables():
    n = np.arange(WIDTH)[:, None]
    analysis = np.zeros((2 * WIDTH, WIDTH))
    for r in range(ROWS):
        analysis[2 * r] = np.cos(2 * np.pi * n[:, 0] * r / WIDTH)
        analysis[2 * r + 1] = np.sin(2 * np.pi * n[:, 0] * r / WIDTH) if r else np.cos(np.pi * n[:, 0])
    a = np.arange(256)[:, None]
    p = np.arange(256)[None, :]
    turn = 2 * np.pi * (a * p % 256) / 256
    first = np.zeros((ROWS, 2, TILES, 4, 256))
    for e in range(2):
        first[:, e, :, 2 * e] = np.cos(turn).reshape(ROWS, TILES, 256)
        first[:, e, :, 2 * e + 1] = -np.sin(turn).reshape(ROWS, TILES, 256)
    first = first.reshape(2 * ROWS * TILES, 4, 2, 128).transpose(2, 0, 1, 3).reshape(2, 2 * ROWS * TILES, 512)
    twist = 2 * np.pi * (a * p) / SEQ
    twist = np.stack([np.cos(twist), -np.sin(twist)], axis=1).reshape(256, 2, 2, 128)
    twist = twist.transpose(2, 0, 1, 3).reshape(2, 256, 256)
    second = np.concatenate([np.cos(turn), np.sin(turn)], axis=1) / np.sqrt(SEQ * WIDTH)
    select = np.zeros((CHANNELS, CHANNELS))
    for r in range(ROWS):
        for ch in range(2):
            for c in range(COLS):
                select[ch * 256 + r * 8 + c, c * WIDTH + partner_channel(r, ch)] = 1.0
    return (
        jnp.asarray(analysis.T, BF16),
        jnp.asarray(first, BF16),
        jnp.asarray(twist, F32),
        jnp.asarray(second, BF16),
        jnp.asarray(select, BF16),
    )


def dot(x, y, dims=((1,), (0,))):
    return lax.dot_general(x, y, (dims, ((), ())), preferred_element_type=F32)


def kernel(
    tokens, gain, w_in, w_gate, w_spec, w_out, analysis, first, twist, second, select,
    out,
    tok, gain_v, w_in_v, wc, w_gate_v, w_spec_v, w_map, w_out_v,
    analysis_v, first_v, twist_v, second_v, select_v,
    turned, send1, recv1, mid, both, sendx, recvx, wide, send2, recv2, sig, result,
    tok_sem, load_sem, s1, r1, sx, rx, s2, r2, so, ro, own_o, swo, rwo, swn, rwn, swy, rwy, sf, rf,
):
    row, col = lax.axis_index("row"), lax.axis_index("col")
    chip, core = col // 2, col % 2

    def cols_of(c):
        return pl.ds(pl.multiple_of(c * OUT, OUT), OUT)

    loads = [
        pltpu.make_async_copy(src, dst, load_sem.at[i])
        for i, (src, dst) in enumerate(
            [
                (analysis, analysis_v), (w_in, w_in_v), (gain, gain_v),
                (first, first_v), (twist, twist_v), (second, second_v),
                (w_gate, w_gate_v), (w_out, w_out_v.at[:, cols_of(col)]),
                (w_spec, w_spec_v), (select, select_v),
            ]
        )
    ]

    def tile_copy(b, j):
        return pltpu.make_async_copy(
            tokens.at[b, pl.ds(pl.multiple_of(j * TILE, TILE), TILE)], tok.at[b, j], tok_sem.at[b, j]
        )

    for i in range(3):
        loads[i].start()

    peers_z = [((row // 4 + dz) % 8) * 4 for dz in range(8)]
    peers_y = [(row % 4 + dy) % 4 for dy in range(4)]
    peers_c = [(col + d) % COLS for d in range(COLS)]
    far_first = sorted(
        ((dz, dy) for dz in range(8) for dy in range(4) if dz or dy),
        key=lambda o: -(min(o[0], 8 - o[0]) + min(o[1], 4 - o[1])),
    )
    paired = []
    for dz, dy in far_first:
        for one in ((dz, dy), (-dz % 8, -dy % 4)):
            if one not in paired:
                paired.append(one)

    barrier = pltpu.get_barrier_semaphore()
    for dz, dy in far_first:
        pl.semaphore_signal(barrier, inc=1, device_id=(peers_z[dz] + peers_y[dy], col), device_id_type=MESH)
    for d in range(1, COLS):
        pl.semaphore_signal(barrier, inc=1, device_id=(row, peers_c[d]), device_id_type=MESH)

    for b in range(SEQS):
        for j in range(TILES):
            tile_copy(b, j).start()
    for i in range(3, 10):
        loads[i].start()

    for i in range(3):
        loads[i].wait()
    scaled = (w_in_v[...].astype(F32) * gain_v[...]).astype(BF16)
    wc[...] = dot(scaled, analysis_v[...], ((0,), (0,))).astype(BF16)

    def rows16(r):
        return pl.ds(pl.multiple_of(16 * r, 16), 16)

    def strided(ref, h, lo, hi, count, stride):
        rows = [ref[h, pl.ds(at, count, stride), :] for at in (lo, hi)]
        return jnp.concatenate(rows, axis=0).astype(BF16)

    def project(b):
        def tiles(i, _):
            for u in range(STEP):
                tile_copy(b, STEP * i + u).wait()
            for u in range(STEP):
                j = STEP * i + u
                t = tok[b, j]
                wide_t = t.astype(F32)
                inverse = lax.rsqrt(jnp.sum(wide_t * wide_t, axis=1, keepdims=True) * (1.0 / D) + EPS)
                flipped = jnp.transpose(dot(t, wc[...]) * inverse)[:WIDTH]
                for h in range(2):
                    turned[h, pl.ds(pl.multiple_of(j * WIDTH, WIDTH), WIDTH), :] = flipped[:, 128 * h : 128 * (h + 1)]
            return 0

        lax.fori_loop(0, TILES // STEP, tiles, 0)

        def pick(i, _):
            for u in range(8):
                r = 8 * i + u
                for h in range(2):
                    lanes = slice(128 * h, 128 * (h + 1))
                    send1[b, rows16(r), lanes] = strided(turned, h, 2 * r, 2 * r + 1, TILES, WIDTH)
            return 0

        lax.fori_loop(0, ROWS // 8, pick, 0)

    def row_send(src, dst, ssem, rsem, block):
        mine = block(row)
        for dz, dy in paired:
            peer = peers_z[dz] + peers_y[dy]
            pltpu.make_async_remote_copy(
                src_ref=src.at[block(peer)], dst_ref=dst.at[mine],
                send_sem=ssem, recv_sem=rsem, device_id=(peer, col), device_id_type=MESH,
            ).start()
        dst[mine] = src[mine]

    def wait_bytes(ref, sem):
        pltpu.make_async_copy(ref, ref, sem).wait()

    most = pl.ds(0, 16 * (ROWS - 1))
    col_order = (4, 5, 3, 2, 6, 7, 1)

    def col_send(b, h):
        for d in col_order:
            peer = peers_c[d]
            pltpu.make_async_remote_copy(
                src_ref=sendx.at[b, h, peer], dst_ref=recvx.at[b, h, col],
                send_sem=sx.at[b, h], recv_sem=rx.at[b, h], device_id=(row, peer), device_id_type=MESH,
            ).start()
        recvx[b, h, col] = sendx[b, h, col]

    def fourier(b):
        lone = row == 0
        across = jnp.transpose(recv1[b])
        for h in range(2):
            y = dot(across, first_v[h])
            tr, ti = twist_v[h, :, :128], twist_v[h, :, 128:]
            ar, ai, br, bi = (y[:, 128 * i : 128 * (i + 1)] for i in range(4))
            pa, qa = ar * tr - ai * ti, ar * ti + ai * tr
            pb, qb = br * tr - bi * ti, br * ti + bi * tr
            both[h, :256, :128] = pa.astype(BF16)
            both[h, 256:, :128] = qa.astype(BF16)
            both[h, :256, 128:] = jnp.where(lone, pb, -qb).astype(BF16)
            both[h, 256:, 128:] = jnp.where(lone, qb, pb).astype(BF16)
            d = dot(second_v[...], both[h])
            da, db = d[:, :128], d[:, 128:]
            mid[h, :256] = jnp.where(lone, da, da - db)
            mid[h, 256:] = jnp.where(lone, db, da + db)
            for c in range(COLS):
                sendx[b, h, c] = strided(mid, h, c, 256 + c, ROWS, COLS)
            col_send(b, h)

    def regroup(b, h):
        for c in range(COLS):
            wide[h, c * WIDTH : (c + 1) * WIDTH, :] = recvx[b, h, c].astype(F32)

        left = lax.broadcasted_iota(jnp.int32, (COLS, 128), 1) < 64

        def pick(i, _):
            for u in range(16):
                r = 16 * i + u
                lo, hi = wide[h, pl.ds(r, COLS, WIDTH), :], wide[h, pl.ds(ROWS + r, COLS, WIDTH), :]
                send2[b, 2 * h, r] = jnp.where(left, lo, pltpu.roll(hi, 64, 1)).astype(BF16)
                send2[b, 2 * h + 1, r] = jnp.where(left, pltpu.roll(lo, 64, 1), hi).astype(BF16)
            return 0

        lax.fori_loop(0, ROWS // 16, pick, 0)

    def gates(b):
        t = tok[b, col].astype(F32)
        inverse = lax.rsqrt(jnp.sum(t * t, axis=1, keepdims=True) * (1.0 / D) + EPS)
        normed = (t * inverse * gain_v[...]).astype(BF16)
        sig[b] = jax.nn.sigmoid(dot(normed, w_gate_v[...]))

    quarter = pl.ds(pl.multiple_of(row % 4 * 256, 256), 256)

    def shard_of(d):
        return cols_of((chip + d) % 4 * 2 + core)

    def share_out(rows, d, ssem, rsem, peer):
        return pltpu.make_async_remote_copy(
            src_ref=w_out_v.at[rows, shard_of(d)], dst_ref=w_out_v.at[rows, shard_of(d)],
            send_sem=ssem, recv_sem=rsem, device_id=peer, device_id_type=MESH,
        )

    def at_chip(d):
        return (row, (chip + d) % 4 * 2 + core)

    every = pl.ds(0, D)
    other_core = (row, chip * 2 + 1 - core)

    def finish(b, t):
        wait_bytes(recv2.at[b, t, pl.ds(0, ROWS - 1)], r2.at[b, t])
        part = pl.ds(64 * t, 64)
        block = jnp.transpose(recv2[b, t].reshape(COLS * ROWS, 128))
        pre = dot(block[:64], w_map[:256]) + dot(block[64:], w_map[256:])
        mixed = (sig[b, part] * pre.astype(BF16).astype(F32)).astype(BF16)
        result[b, part] = dot(mixed, w_out_v[...]).astype(BF16)
        place = pl.ds(pl.multiple_of(col * TILE + 64 * t, 64), 64)

        for d in col_order:
            peer = peers_c[d]
            pltpu.make_async_remote_copy(
                src_ref=result.at[b, part, cols_of(peer)], dst_ref=out.at[b, place],
                send_sem=so.at[b, t], recv_sem=ro.at[b, t], device_id=(row, peer), device_id_type=MESH,
            ).start()
        pltpu.make_async_copy(result.at[b, part, cols_of(col)], out.at[b, place], own_o.at[b, t]).start()

    def forward(b):
        row_send(send1.at[b], recv1.at[b], s1.at[b], r1.at[b], rows16)

    def back(b, h):
        wait_bytes(recvx.at[b, h, pl.ds(0, COLS - 1)], rx.at[b, h])
        regroup(b, h)
        for t in (2 * h, 2 * h + 1):
            row_send(send2.at[b, t], recv2.at[b, t], s2.at[b, t], r2.at[b, t], lambda r: r)

    project(0)
    pl.semaphore_wait(barrier, ROWS - 1 + COLS - 1)
    forward(0)
    loads[7].wait()
    share_out(quarter, 0, swo, rwo, at_chip(2)).start()
    share_out(every, 0, swn, rwn, at_chip(1)).start()
    share_out(every, 0, swn, rwn, at_chip(3)).start()
    share_out(every, 0, sf, rf, other_core).start()
    project(1)
    loads[6].wait()
    gates(0)
    loads[8].wait()
    loads[9].wait()
    w_map[...] = dot(select_v[...], w_spec_v[...]).astype(BF16)
    gates(1)
    forward(1)
    wait_bytes(w_out_v.at[pl.ds(0, 256), pl.ds(0, OUT)], rwo)
    for d in range(1, 4):
        share_out(quarter, 2, swy, rwy, (row // 4 * 4 + (row % 4 + d) % 4, col)).start()
    for i in range(3, 6):
        loads[i].wait()

    wait_bytes(recv1.at[0, most], r1.at[0])
    fourier(0)
    back(0, 0)
    wait_bytes(recv1.at[1, most], r1.at[1])
    fourier(1)
    back(0, 1)
    wait_bytes(w_out_v.at[:, pl.ds(0, 2 * OUT)], rwn)
    wait_bytes(w_out_v.at[pl.ds(0, 768), pl.ds(0, OUT)], rwy)
    for d in range(1, 4):
        share_out(every, d, sf, rf, other_core).start()
    back(1, 0)
    wait_bytes(w_out_v.at[:, pl.ds(0, 4 * OUT)], rf)
    finish(0, 0)
    back(1, 1)
    for b, t in ((0, 1), (0, 2), (0, 3), (1, 0), (1, 1), (1, 2), (1, 3)):
        finish(b, t)

    wait_bytes(w_out_v.at[pl.ds(0, 256), pl.ds(0, OUT)], swo)
    wait_bytes(w_out_v.at[:, pl.ds(0, 2 * OUT)], swn)
    wait_bytes(w_out_v.at[pl.ds(0, 768), pl.ds(0, OUT)], swy)
    wait_bytes(w_out_v.at[:, pl.ds(0, 4 * OUT)], sf)
    for b in range(SEQS):
        wait_bytes(send1.at[b, most], s1.at[b])
        for h in range(2):
            wait_bytes(sendx.at[b, h, pl.ds(0, COLS - 1)], sx.at[b, h])
        for t in range(4):
            part = pl.ds(64 * t, 64)
            wait_bytes(send2.at[b, t, pl.ds(0, ROWS - 1)], s2.at[b, t])
            wait_bytes(result.at[b, part, pl.ds(0, (COLS - 1) * OUT)], so.at[b, t])
            wait_bytes(out.at[b, pl.ds(0, (COLS - 1) * 64)], ro.at[b, t])
            wait_bytes(result.at[b, part, pl.ds(0, OUT)], own_o.at[b, t])


def on_device(tokens, norm_gain, w_fourier_in, w_gate, w_spectrum, w_output):
    dma = pltpu.SemaphoreType.DMA
    pair, halves, quarters = dma((SEQS,)), dma((SEQS, 2)), dma((SEQS, 4))
    scratch = [
        pltpu.VMEM((SEQS, TILES, TILE, D), BF16),
        pltpu.VMEM((1, D), F32),
        pltpu.VMEM((WIDTH, D), BF16),
        pltpu.VMEM((D, 2 * WIDTH), BF16),
        pltpu.VMEM((D, D), BF16),
        pltpu.VMEM((CHANNELS, D), BF16),
        pltpu.VMEM((CHANNELS, D), BF16),
        pltpu.VMEM((D, D), BF16),
        pltpu.VMEM((WIDTH, 2 * WIDTH), BF16),
        pltpu.VMEM((2, 512, 512), BF16),
        pltpu.VMEM((2, 256, 256), F32),
        pltpu.VMEM((256, 512), BF16),
        pltpu.VMEM((CHANNELS, CHANNELS), BF16),
        pltpu.VMEM((2, TILES * WIDTH, 128), F32),
        pltpu.VMEM((SEQS, 16 * ROWS, 256), BF16),
        pltpu.VMEM((SEQS, 16 * ROWS, 256), BF16),
        pltpu.VMEM((2, 512, 128), F32),
        pltpu.VMEM((2, 512, 256), BF16),
        pltpu.VMEM((SEQS, 2, COLS, WIDTH, 128), BF16),
        pltpu.VMEM((SEQS, 2, COLS, WIDTH, 128), BF16),
        pltpu.VMEM((2, COLS * WIDTH, 128), F32),
        pltpu.VMEM((SEQS, 4, ROWS, 8, 128), BF16),
        pltpu.VMEM((SEQS, 4, ROWS, 8, 128), BF16),
        pltpu.VMEM((SEQS, TILE, D), F32),
        pltpu.VMEM((SEQS, TILE, D), BF16),
        dma((SEQS, TILES)), dma((10,)),
        pair, pair, halves, halves, quarters, quarters, quarters, quarters, quarters,
        dma, dma, dma, dma, dma, dma, dma, dma,
    ]
    anywhere = pl.BlockSpec(memory_space=pl.ANY)
    return pl.pallas_call(
        kernel,
        out_shape=pltpu.VMEM((SEQS, LOCAL, OUT), BF16),
        in_specs=[anywhere] * 11,
        out_specs=anywhere,
        scratch_shapes=scratch,
        compiler_params=pltpu.CompilerParams(
            collective_id=0, has_side_effects=True, vmem_limit_bytes=56 * 1024 * 1024
        ),
        name="fourier_mix",
    )(tokens, norm_gain.reshape(1, D), w_fourier_in.T, w_gate, w_spectrum, w_output, *tables())


def solution(mesh):
    placed = (P(None, "row", None), P(), P(None, "col"), P(), P(), P(None, "col"))
    return jax.shard_map(
        on_device, mesh=mesh, in_specs=placed, out_specs=P(None, "row", "col"), check_vma=False
    )
```

```python
import numpy as np
import jax
import jax.numpy as jnp
from jax import lax
from jax.experimental import pallas as pl
from jax.experimental.pallas import tpu as pltpu
from jax.sharding import PartitionSpec as P

MESH = pl.DeviceIdType.MESH
ROWS, COLS = 32, 8
SEQS, LOCAL, D = 2, 2048, 1024
TILE = 256
TILES = LOCAL // TILE
STEP = 2
SEQ = ROWS * LOCAL
WIDTH = 64
CHANNELS = COLS * WIDTH
OUT = D // COLS
EPS = 1e-6
F32, BF16 = jnp.float32, jnp.bfloat16


def partner_channel(r, second):
    if r == 0:
        return 32 * second
    return WIDTH - r if second else r


def tables():
    n = np.arange(WIDTH)[:, None]
    analysis = np.zeros((2 * WIDTH, WIDTH))
    for r in range(ROWS):
        analysis[2 * r] = np.cos(2 * np.pi * n[:, 0] * r / WIDTH)
        analysis[2 * r + 1] = np.sin(2 * np.pi * n[:, 0] * r / WIDTH) if r else np.cos(np.pi * n[:, 0])
    a = np.arange(256)[:, None]
    p = np.arange(256)[None, :]
    turn = 2 * np.pi * (a * p % 256) / 256
    first = np.zeros((ROWS, 2, TILES, 4, 256))
    for e in range(2):
        first[:, e, :, 2 * e] = np.cos(turn).reshape(ROWS, TILES, 256)
        first[:, e, :, 2 * e + 1] = -np.sin(turn).reshape(ROWS, TILES, 256)
    first = first.reshape(2 * ROWS * TILES, 4, 2, 128).transpose(2, 0, 1, 3).reshape(2, 2 * ROWS * TILES, 512)
    twist = 2 * np.pi * (a * p) / SEQ
    twist = np.stack([np.cos(twist), -np.sin(twist)], axis=1).reshape(256, 2, 2, 128)
    twist = twist.transpose(2, 0, 1, 3).reshape(2, 256, 256)
    second = np.concatenate([np.cos(turn), np.sin(turn)], axis=1) / np.sqrt(SEQ * WIDTH)
    select = np.zeros((CHANNELS, CHANNELS))
    for r in range(ROWS):
        for ch in range(2):
            for c in range(COLS):
                select[ch * 256 + r * 8 + c, c * WIDTH + partner_channel(r, ch)] = 1.0
    return (
        jnp.asarray(analysis.T, BF16),
        jnp.asarray(first, BF16),
        jnp.asarray(twist, F32),
        jnp.asarray(second, BF16),
        jnp.asarray(select, BF16),
    )


def dot(x, y, dims=((1,), (0,))):
    return lax.dot_general(x, y, (dims, ((), ())), preferred_element_type=F32)


def kernel(
    tokens, gain, w_in, w_gate, w_spec, w_out, analysis, first, twist, second, select,
    out,
    tok, gain_v, w_in_v, wc, w_gate_v, w_spec_v, w_map, w_out_v,
    analysis_v, first_v, twist_v, second_v, select_v,
    turned, send1, recv1, mid, both, sendx, recvx, wide, send2, recv2, sig, result,
    tok_sem, load_sem, s1, r1, sx, rx, s2, r2, so, ro, own_o, swo, rwo, swn, rwn, swy, rwy, sf, rf,
):
    row, col = lax.axis_index("row"), lax.axis_index("col")
    chip, core = col // 2, col % 2

    def cols_of(c):
        return pl.ds(pl.multiple_of(c * OUT, OUT), OUT)

    loads = [
        pltpu.make_async_copy(src, dst, load_sem.at[i])
        for i, (src, dst) in enumerate(
            [
                (analysis, analysis_v), (w_in, w_in_v), (gain, gain_v),
                (first, first_v), (twist, twist_v), (second, second_v),
                (w_gate, w_gate_v), (w_out, w_out_v.at[:, cols_of(col)]),
                (w_spec, w_spec_v), (select, select_v),
            ]
        )
    ]

    def tile_copy(b, j):
        return pltpu.make_async_copy(
            tokens.at[b, pl.ds(pl.multiple_of(j * TILE, TILE), TILE)], tok.at[b, j], tok_sem.at[b, j]
        )

    for i in range(3):
        loads[i].start()

    peers_z = [((row // 4 + dz) % 8) * 4 for dz in range(8)]
    peers_y = [(row % 4 + dy) % 4 for dy in range(4)]
    peers_c = [(col + d) % COLS for d in range(COLS)]
    far_first = sorted(
        ((dz, dy) for dz in range(8) for dy in range(4) if dz or dy),
        key=lambda o: -(min(o[0], 8 - o[0]) + min(o[1], 4 - o[1])),
    )
    paired = []
    for dz, dy in far_first:
        for one in ((dz, dy), (-dz % 8, -dy % 4)):
            if one not in paired:
                paired.append(one)

    barrier = pltpu.get_barrier_semaphore()
    for dz, dy in far_first:
        pl.semaphore_signal(barrier, inc=1, device_id=(peers_z[dz] + peers_y[dy], col), device_id_type=MESH)
    for d in range(1, COLS):
        pl.semaphore_signal(barrier, inc=1, device_id=(row, peers_c[d]), device_id_type=MESH)

    for b in range(SEQS):
        for j in range(TILES):
            tile_copy(b, j).start()
    for i in range(3, 10):
        loads[i].start()

    for i in range(3):
        loads[i].wait()
    scaled = (w_in_v[...].astype(F32) * gain_v[...]).astype(BF16)
    wc[...] = dot(scaled, analysis_v[...], ((0,), (0,))).astype(BF16)

    def rows16(r):
        return pl.ds(pl.multiple_of(16 * r, 16), 16)

    def strided(ref, h, lo, hi, count, stride):
        rows = [ref[h, pl.ds(at, count, stride), :] for at in (lo, hi)]
        return jnp.concatenate(rows, axis=0).astype(BF16)

    def project(b):
        def tiles(i, _):
            for u in range(STEP):
                tile_copy(b, STEP * i + u).wait()
            for u in range(STEP):
                j = STEP * i + u
                t = tok[b, j]
                wide_t = t.astype(F32)
                inverse = lax.rsqrt(jnp.sum(wide_t * wide_t, axis=1, keepdims=True) * (1.0 / D) + EPS)
                flipped = jnp.transpose(dot(t, wc[...]) * inverse)[:WIDTH]
                for h in range(2):
                    turned[h, pl.ds(pl.multiple_of(j * WIDTH, WIDTH), WIDTH), :] = flipped[:, 128 * h : 128 * (h + 1)]
            return 0

        lax.fori_loop(0, TILES // STEP, tiles, 0)

        def pick(i, _):
            for u in range(8):
                r = 8 * i + u
                for h in range(2):
                    lanes = slice(128 * h, 128 * (h + 1))
                    send1[b, rows16(r), lanes] = strided(turned, h, 2 * r, 2 * r + 1, TILES, WIDTH)
            return 0

        lax.fori_loop(0, ROWS // 8, pick, 0)

    def row_send(src, dst, ssem, rsem, block):
        mine = block(row)
        for dz, dy in paired:
            peer = peers_z[dz] + peers_y[dy]
            pltpu.make_async_remote_copy(
                src_ref=src.at[block(peer)], dst_ref=dst.at[mine],
                send_sem=ssem, recv_sem=rsem, device_id=(peer, col), device_id_type=MESH,
            ).start()
        dst[mine] = src[mine]

    def wait_bytes(ref, sem):
        pltpu.make_async_copy(ref, ref, sem).wait()

    most = pl.ds(0, 16 * (ROWS - 1))
    col_order = (4, 5, 3, 2, 6, 7, 1)

    def col_send(b, h):
        for d in col_order:
            peer = peers_c[d]
            pltpu.make_async_remote_copy(
                src_ref=sendx.at[b, h, peer], dst_ref=recvx.at[b, h, col],
                send_sem=sx.at[b, h], recv_sem=rx.at[b, h], device_id=(row, peer), device_id_type=MESH,
            ).start()
        recvx[b, h, col] = sendx[b, h, col]

    def fourier(b):
        lone = row == 0
        across = jnp.transpose(recv1[b])
        for h in range(2):
            y = dot(across, first_v[h])
            tr, ti = twist_v[h, :, :128], twist_v[h, :, 128:]
            ar, ai, br, bi = (y[:, 128 * i : 128 * (i + 1)] for i in range(4))
            pa, qa = ar * tr - ai * ti, ar * ti + ai * tr
            pb, qb = br * tr - bi * ti, br * ti + bi * tr
            both[h, :256, :128] = pa.astype(BF16)
            both[h, 256:, :128] = qa.astype(BF16)
            both[h, :256, 128:] = jnp.where(lone, pb, -qb).astype(BF16)
            both[h, 256:, 128:] = jnp.where(lone, qb, pb).astype(BF16)
            d = dot(second_v[...], both[h])
            da, db = d[:, :128], d[:, 128:]
            mid[h, :256] = jnp.where(lone, da, da - db)
            mid[h, 256:] = jnp.where(lone, db, da + db)
            for c in range(COLS):
                sendx[b, h, c] = strided(mid, h, c, 256 + c, ROWS, COLS)
            col_send(b, h)

    def regroup(b, h):
        for c in range(COLS):
            wide[h, c * WIDTH : (c + 1) * WIDTH, :] = recvx[b, h, c].astype(F32)

        left = lax.broadcasted_iota(jnp.int32, (COLS, 128), 1) < 64

        def pick(i, _):
            for u in range(16):
                r = 16 * i + u
                lo, hi = wide[h, pl.ds(r, COLS, WIDTH), :], wide[h, pl.ds(ROWS + r, COLS, WIDTH), :]
                send2[b, 2 * h, r] = jnp.where(left, lo, pltpu.roll(hi, 64, 1)).astype(BF16)
                send2[b, 2 * h + 1, r] = jnp.where(left, pltpu.roll(lo, 64, 1), hi).astype(BF16)
            return 0

        lax.fori_loop(0, ROWS // 16, pick, 0)

    def gates(b):
        t = tok[b, col].astype(F32)
        inverse = lax.rsqrt(jnp.sum(t * t, axis=1, keepdims=True) * (1.0 / D) + EPS)
        normed = (t * inverse * gain_v[...]).astype(BF16)
        sig[b] = jax.nn.sigmoid(dot(normed, w_gate_v[...]))

    quarter = pl.ds(pl.multiple_of(row % 4 * 256, 256), 256)

    def shard_of(d):
        return cols_of((chip + d) % 4 * 2 + core)

    def share_out(rows, d, ssem, rsem, peer):
        return pltpu.make_async_remote_copy(
            src_ref=w_out_v.at[rows, shard_of(d)], dst_ref=w_out_v.at[rows, shard_of(d)],
            send_sem=ssem, recv_sem=rsem, device_id=peer, device_id_type=MESH,
        )

    def at_chip(d):
        return (row, (chip + d) % 4 * 2 + core)

    every = pl.ds(0, D)
    other_core = (row, chip * 2 + 1 - core)

    def finish(b, t):
        wait_bytes(recv2.at[b, t, pl.ds(0, ROWS - 1)], r2.at[b, t])
        part = pl.ds(64 * t, 64)
        block = jnp.transpose(recv2[b, t].reshape(COLS * ROWS, 128))
        pre = dot(block[:64], w_map[:256]) + dot(block[64:], w_map[256:])
        mixed = (sig[b, part] * pre.astype(BF16).astype(F32)).astype(BF16)
        result[b, part] = dot(mixed, w_out_v[...]).astype(BF16)
        place = pl.ds(pl.multiple_of(col * TILE + 64 * t, 64), 64)

        for d in col_order:
            peer = peers_c[d]
            pltpu.make_async_remote_copy(
                src_ref=result.at[b, part, cols_of(peer)], dst_ref=out.at[b, place],
                send_sem=so.at[b, t], recv_sem=ro.at[b, t], device_id=(row, peer), device_id_type=MESH,
            ).start()
        pltpu.make_async_copy(result.at[b, part, cols_of(col)], out.at[b, place], own_o.at[b, t]).start()

    def forward(b):
        row_send(send1.at[b], recv1.at[b], s1.at[b], r1.at[b], rows16)

    def back(b, h):
        wait_bytes(recvx.at[b, h, pl.ds(0, COLS - 1)], rx.at[b, h])
        regroup(b, h)
        for t in (2 * h, 2 * h + 1):
            row_send(send2.at[b, t], recv2.at[b, t], s2.at[b, t], r2.at[b, t], lambda r: r)

    project(0)
    pl.semaphore_wait(barrier, ROWS - 1 + COLS - 1)
    forward(0)
    loads[7].wait()
    share_out(quarter, 0, swo, rwo, at_chip(2)).start()
    share_out(every, 0, swn, rwn, at_chip(1)).start()
    share_out(every, 0, swn, rwn, at_chip(3)).start()
    share_out(every, 0, sf, rf, other_core).start()
    project(1)
    loads[6].wait()
    gates(0)
    loads[8].wait()
    loads[9].wait()
    w_map[...] = dot(select_v[...], w_spec_v[...]).astype(BF16)
    gates(1)
    forward(1)
    wait_bytes(w_out_v.at[pl.ds(0, 256), pl.ds(0, OUT)], rwo)
    for d in range(1, 4):
        share_out(quarter, 2, swy, rwy, (row // 4 * 4 + (row % 4 + d) % 4, col)).start()
    for i in range(3, 6):
        loads[i].wait()

    wait_bytes(recv1.at[0, most], r1.at[0])
    fourier(0)
    back(0, 0)
    wait_bytes(recv1.at[1, most], r1.at[1])
    fourier(1)
    back(0, 1)
    wait_bytes(w_out_v.at[:, pl.ds(0, 2 * OUT)], rwn)
    wait_bytes(w_out_v.at[pl.ds(0, 768), pl.ds(0, OUT)], rwy)
    for d in range(1, 4):
        share_out(every, d, sf, rf, other_core).start()
    back(1, 0)
    wait_bytes(w_out_v.at[:, pl.ds(0, 4 * OUT)], rf)
    finish(0, 0)
    finish(0, 1)
    back(1, 1)
    for b, t in ((0, 2), (0, 3), (1, 0), (1, 1), (1, 2), (1, 3)):
        finish(b, t)

    wait_bytes(w_out_v.at[pl.ds(0, 256), pl.ds(0, OUT)], swo)
    wait_bytes(w_out_v.at[:, pl.ds(0, 2 * OUT)], swn)
    wait_bytes(w_out_v.at[pl.ds(0, 768), pl.ds(0, OUT)], swy)
    wait_bytes(w_out_v.at[:, pl.ds(0, 4 * OUT)], sf)
    for b in range(SEQS):
        wait_bytes(send1.at[b, most], s1.at[b])
        for h in range(2):
            wait_bytes(sendx.at[b, h, pl.ds(0, COLS - 1)], sx.at[b, h])
        for t in range(4):
            part = pl.ds(64 * t, 64)
            wait_bytes(send2.at[b, t, pl.ds(0, ROWS - 1)], s2.at[b, t])
            wait_bytes(result.at[b, part, pl.ds(0, (COLS - 1) * OUT)], so.at[b, t])
            wait_bytes(out.at[b, pl.ds(0, (COLS - 1) * 64)], ro.at[b, t])
            wait_bytes(result.at[b, part, pl.ds(0, OUT)], own_o.at[b, t])


def on_device(tokens, norm_gain, w_fourier_in, w_gate, w_spectrum, w_output):
    dma = pltpu.SemaphoreType.DMA
    pair, halves, quarters = dma((SEQS,)), dma((SEQS, 2)), dma((SEQS, 4))
    scratch = [
        pltpu.VMEM((SEQS, TILES, TILE, D), BF16),
        pltpu.VMEM((1, D), F32),
        pltpu.VMEM((WIDTH, D), BF16),
        pltpu.VMEM((D, 2 * WIDTH), BF16),
        pltpu.VMEM((D, D), BF16),
        pltpu.VMEM((CHANNELS, D), BF16),
        pltpu.VMEM((CHANNELS, D), BF16),
        pltpu.VMEM((D, D), BF16),
        pltpu.VMEM((WIDTH, 2 * WIDTH), BF16),
        pltpu.VMEM((2, 512, 512), BF16),
        pltpu.VMEM((2, 256, 256), F32),
        pltpu.VMEM((256, 512), BF16),
        pltpu.VMEM((CHANNELS, CHANNELS), BF16),
        pltpu.VMEM((2, TILES * WIDTH, 128), F32),
        pltpu.VMEM((SEQS, 16 * ROWS, 256), BF16),
        pltpu.VMEM((SEQS, 16 * ROWS, 256), BF16),
        pltpu.VMEM((2, 512, 128), F32),
        pltpu.VMEM((2, 512, 256), BF16),
        pltpu.VMEM((SEQS, 2, COLS, WIDTH, 128), BF16),
        pltpu.VMEM((SEQS, 2, COLS, WIDTH, 128), BF16),
        pltpu.VMEM((2, COLS * WIDTH, 128), F32),
        pltpu.VMEM((SEQS, 4, ROWS, 8, 128), BF16),
        pltpu.VMEM((SEQS, 4, ROWS, 8, 128), BF16),
        pltpu.VMEM((SEQS, TILE, D), F32),
        pltpu.VMEM((SEQS, TILE, D), BF16),
        dma((SEQS, TILES)), dma((10,)),
        pair, pair, halves, halves, quarters, quarters, quarters, quarters, quarters,
        dma, dma, dma, dma, dma, dma, dma, dma,
    ]
    anywhere = pl.BlockSpec(memory_space=pl.ANY)
    return pl.pallas_call(
        kernel,
        out_shape=pltpu.VMEM((SEQS, LOCAL, OUT), BF16),
        in_specs=[anywhere] * 11,
        out_specs=anywhere,
        scratch_shapes=scratch,
        compiler_params=pltpu.CompilerParams(
            collective_id=0, has_side_effects=True, vmem_limit_bytes=56 * 1024 * 1024
        ),
        name="fourier_mix",
    )(tokens, norm_gain.reshape(1, D), w_fourier_in.T, w_gate, w_spectrum, w_output, *tables())


def solution(mesh):
    placed = (P(None, "row", None), P(), P(None, "col"), P(), P(), P(None, "col"))
    return jax.shard_map(
        on_device, mesh=mesh, in_specs=placed, out_specs=P(None, "row", "col"), check_vma=False
    )
```
